512 devices in a mesh: fs: 64 (over z, y), tp: 8 (over x, core).
Axes of the slice: x: 4, y: 8, z: 8, core: 2. Of those that a mesh axis runs over, the one named last changes fastest.
Arguments:
- tokens: bfloat16 [12288, 2048], P('fs'), may hold values from -6 to 6
- route_ids: int32 [12288, 2], P('fs'), may hold values from 0 to 7, all different within a row; in each aligned block of 192 rows (0 to 191, 192 to 383, ...) at most 96 rows name the same one
- route_logits: float32 [12288, 2], P('fs'), may hold values from -6 to 6
- norm_gain: float32 [2048], P('fs'), may hold values from 0.1 to 1.9
- gate_weight: float32 [8, 2048, 2048], P(None, 'fs', 'tp'), may hold values from -0.125 to 0.125
- up_weight: float32 [8, 2048, 2048], P(None, 'fs', 'tp'), may hold values from -0.125 to 0.125
- down_weight: float32 [8, 2048, 2048], P(None, 'fs', 'tp'), may hold values from -0.125 to 0.125
Outputs:
- mixed: bfloat16 [12288, 2048], P('fs')
- gate_copies: bfloat16 [64, 2048, 2048], P('fs', None, 'tp')
- up_copies: bfloat16 [64, 2048, 2048], P('fs', None, 'tp')
- down_copies: bfloat16 [64, 2048, 2048], P('fs', None, 'tp')
The draws below stay inside these ranges and needn't reach their ends.
Inputs may be any that keep to these rules, and one draw needn't show every extreme that they name: `route_ids`: each row names 2 different experts. Among the rows of one index of fs no expert is named by more than 96 rows, a bound that some of them reach.
All inputs are finite; a program needn't handle non-finite values.
Results may differ from the reference program's by a relative error of at most 0.014.
Values may be sent and summed in bfloat16 or wider, within the bound.
No kernel may reach another device: no remote copies, remote signals or barrier semaphores. Data moves between devices by JAX's collectives and lax.ppermute only.
A program may use at most 64 MiB of HBM per device.

```python
import math
import jax
import jax.numpy as jnp
import numpy as np
from jax import lax

D = 2048
FF = 2048
EXPERTS = 8
TOP = 2
TOK_DEV = 192
CAP = 96
TOKENS = 12288
N_FS = 64
N_TP = 8


def levels(key, extent, split, low, high):
    def one(dim, blocks):
        steps = jax.random.uniform(jax.random.fold_in(jax.random.fold_in(key, 6), dim), (blocks,), jnp.float32, low / len(split), high / len(split))
        return jnp.repeat(jnp.exp(steps), extent[dim] // blocks).reshape((-1,) + (1,) * (len(extent) - dim - 1))

    level = one(*split[0])
    for cut in split[1:]:
        level = level * one(*cut)
    return level


def deal_out(rng, own, number, rows, number_of, top, most, lean):
    ranking = jax.random.permutation(rng, number_of)
    packed, usual = load_shares(number_of, rows * top, most, lean, True), load_shares(number_of, rows * top, most, lean, False)
    places = jnp.arange(number_of)

    def named(tallies, rotation):
        used = int((tallies > 0).sum())
        fixed = max(1, used // 4)
        moved = fixed + (places - fixed + rotation * (used - fixed)) % max(1, number_of - fixed)
        return jnp.zeros((number_of,), jnp.int32).at[ranking[jnp.where(places < fixed, places, moved)]].set(jnp.asarray(tallies, jnp.int32))

    tallies = jnp.where(number % 4 == 0, named(packed, number // 4), named(usual, number - number // 4 - 1))
    mixed = jax.random.permutation(jax.random.fold_in(own, 3), number_of)
    donor, sink = mixed[0:number_of // 2 * 2:2], mixed[1:number_of // 2 * 2:2]
    margin = jnp.minimum(tallies[donor] - 1, most - tallies[sink]) // 2
    margin = jnp.where((donor == ranking[0]) | (sink == ranking[0]) | (tallies[sink] == 0), 0, jnp.maximum(margin, 0))
    moved = jax.random.randint(jax.random.fold_in(own, 4), (number_of // 2,), 0, 1 << 20) % (margin + 1)
    tallies = tallies.at[donor].add(-moved).at[sink].add(moved)
    labels = jnp.searchsorted(jnp.cumsum(tallies), jnp.arange(rows * top), side="right").astype(jnp.int32)
    grid = labels.reshape(top, rows).T
    grid = grid[jax.random.permutation(jax.random.fold_in(own, 1), rows)]
    rotation = jax.random.randint(jax.random.fold_in(own, 2), (rows, 1), 0, top)
    return jnp.take_along_axis(grid, (jnp.arange(top)[None, :] + rotation) % top, axis=1)


def load_shares(amount, total, reach, skew, full):
    weights = [(1 << 20) // math.isqrt(rank ** skew) + 1 for rank in range(1, amount + 1)]
    largest = reach if full else min(reach, max(-(-total // amount), total * weights[0] // sum(weights)))
    least = 1 if total - largest >= amount - 1 else 0
    given, rest = [largest] + [least] * (amount - 1), total - largest - least * (amount - 1)
    while rest > 0:
        candidates = [i for i in range(1, amount) if given[i] < largest] or [i for i in range(1, amount) if given[i] < reach]
        pool, left = sum([weights[i] for i in candidates]), rest
        for i in candidates:
            more = min(reach - given[i], max(1, left * weights[i] // pool), rest)
            given[i] = given[i] + more
            rest = rest - more
    return np.array(given)


def centred(stream_key, extent, deviation, limit, cuts=(), held_as=jnp.bfloat16):
    result = deviation * jax.random.normal(stream_key, extent, jnp.float32)
    if cuts:
        result = result * levels(stream_key, extent, cuts, -0.22, 0.18)
    return jnp.clip(result, -limit, limit).astype(held_as)


def setup_inputs(seed: int = 0) -> dict:
    seeds = jax.random.split(jax.random.key(seed), 8)
    tokens = centred(seeds[0], (TOKENS, D), 1.0, 6.0, ((0, 64),))
    route_ids_keys = jax.random.split(jax.random.fold_in(seeds[1], 1), TOKENS // TOK_DEV)
    route_ids_turns = jax.random.permutation(jax.random.fold_in(seeds[1], 3), TOKENS // TOK_DEV)
    route_ids = jax.vmap(lambda own, number: deal_out(jax.random.fold_in(seeds[1], 2), own, number, TOK_DEV, EXPERTS, TOP, CAP, 1))(route_ids_keys, route_ids_turns).reshape((TOKENS, TOP))
    route_logits = centred(seeds[2], (TOKENS, TOP), 1.5, 6.0, ((0, 64),), jnp.float32)
    norm_gain = jnp.clip(1.0 + 0.18 * jax.random.normal(seeds[3], (D,), jnp.float32), 0.1, 1.9)
    gate_weight = centred(seeds[4], (EXPERTS, D, FF), D ** -0.5, 0.125, ((1, 64), (2, 8)), jnp.float32)
    up_weight = centred(seeds[5], (EXPERTS, D, FF), D ** -0.5, 0.125, ((1, 64), (2, 8)), jnp.float32)
    down_weight = centred(seeds[6], (EXPERTS, D, FF), FF ** -0.5, 0.125, ((1, 64), (2, 8)), jnp.float32)
    return dict(tokens=tokens, route_ids=route_ids, route_logits=route_logits, norm_gain=norm_gain, gate_weight=gate_weight, up_weight=up_weight, down_weight=down_weight)


def expert_rows(rows, gate_matrix, up_matrix, down_matrix):
    gate_act = jnp.dot(rows, gate_matrix, preferred_element_type=jnp.float32)
    up_act = jnp.dot(rows, up_matrix, preferred_element_type=jnp.float32)
    hidden = (jax.nn.silu(gate_act) * up_act).astype(jnp.bfloat16)
    row_count = rows.shape[0]
    blocks = hidden.reshape(row_count, N_TP, FF // N_TP).astype(jnp.float32)
    down_blocks = down_matrix.reshape(D, N_TP, FF // N_TP).astype(jnp.float32)
    partial_value = jnp.einsum('rbf,dbf->brd', blocks, down_blocks)
    rounded = lax.optimization_barrier(partial_value.astype(jnp.bfloat16))
    return lax.optimization_barrier(jnp.sum(rounded.astype(jnp.float32), axis=0)).astype(jnp.bfloat16)

def reference(tokens, route_ids, route_logits, norm_gain, gate_weight, up_weight, down_weight):
    copies = N_FS // EXPERTS
    folded_gate = (norm_gain[None, :, None] * gate_weight).astype(jnp.bfloat16)
    folded_up = (norm_gain[None, :, None] * up_weight).astype(jnp.bfloat16)
    down_cast = down_weight.astype(jnp.bfloat16)
    gate_copies = jnp.repeat(folded_gate, copies, axis=0)
    up_copies = jnp.repeat(folded_up, copies, axis=0)
    down_copies = jnp.repeat(down_cast, copies, axis=0)
    values = tokens.astype(jnp.float32)
    center = lax.optimization_barrier(jnp.mean(values, axis=1, keepdims=True))
    spread = lax.optimization_barrier(jnp.mean(jnp.square(values - center), axis=1, keepdims=True))
    normed = ((values - center) * lax.rsqrt(spread + 1e-06)).astype(jnp.bfloat16)
    per_source = route_ids.reshape(N_FS, TOK_DEV * TOP)
    onehot_table = (per_source[:, :, None] == jnp.arange(EXPERTS, dtype=jnp.int32)[None, None, :]).astype(jnp.int32)
    before = jnp.cumsum(onehot_table, axis=1) - onehot_table
    order_rank = lax.optimization_barrier(jnp.sum(before * onehot_table, axis=2))
    source = jnp.arange(N_FS, dtype=jnp.int32)[:, None]
    position = source * CAP + order_rank
    owners = source * TOK_DEV + jnp.arange(TOK_DEV * TOP, dtype=jnp.int32)[None, :] // TOP
    slot_token = jnp.full((EXPERTS, N_FS * CAP), TOKENS, jnp.int32).at[per_source, position].set(owners)
    padded = jnp.concatenate([normed, jnp.zeros((1, D), jnp.bfloat16)], axis=0)

    def one_expert(index):
        rows = padded[slot_token[index]]
        return expert_rows(rows, folded_gate[index], folded_up[index], down_cast[index])
    results = lax.map(one_expert, jnp.arange(EXPERTS, dtype=jnp.int32))
    picked = results[per_source, position].reshape(TOKENS, TOP, D).astype(jnp.float32)
    first_weight = jax.nn.sigmoid(route_logits[:, 0] - route_logits[:, 1])
    second_weight = jax.nn.sigmoid(route_logits[:, 1] - route_logits[:, 0])
    mixed = (first_weight[:, None] * picked[:, 0] + second_weight[:, None] * picked[:, 1]).astype(jnp.bfloat16)
    return (mixed, gate_copies, up_copies, down_copies)
```

```python
import functools

import jax
import jax.numpy as jnp
from jax import lax
from jax.experimental import pallas as pl
from jax.experimental.pallas import tpu as pltpu
from jax.sharding import Mesh
from jax.sharding import PartitionSpec as P

CAP = 96
BF16 = jnp.bfloat16
F32 = jnp.float32
VMEM = pl.BlockSpec(memory_space=pltpu.VMEM)
SMEM = pl.BlockSpec(memory_space=pltpu.SMEM)
ANY = pl.BlockSpec(memory_space=pl.ANY)


def shift(value, axis, by):
    size = lax.axis_size(axis)
    return lax.ppermute(value, axis, [(i, (i + by) % size) for i in range(size)])


def swap(value):
    return lax.ppermute(value, "c", [(0, 1), (1, 0)])


def dispatch_kernel(experts, place, ids_ref, tokens_ref, out_ref):
    rows = tokens_ref.shape[0]
    values = tokens_ref[...].astype(F32)
    center = jnp.mean(values, axis=1, keepdims=True)
    spread = jnp.mean(jnp.square(values - center), axis=1, keepdims=True)
    start = pl.multiple_of((place[1] * 4 + place[0]) * 256, 256)
    own = tokens_ref[:, pl.ds(start, 256)].astype(F32)
    normed = ((own - center) * lax.rsqrt(spread + 1e-06)).astype(BF16)
    first, second = ids_ref[0:1, :], ids_ref[1:2, :]
    expert = lax.broadcasted_iota(jnp.int32, (experts, rows), 0)
    chosen = jnp.where((expert == first) | (expert == second), 1.0, 0.0)
    earlier = jnp.where(
        lax.broadcasted_iota(jnp.int32, (rows, rows), 0)
        < lax.broadcasted_iota(jnp.int32, (rows, rows), 1),
        1.0,
        0.0,
    )
    rank = jnp.dot(chosen.astype(BF16), earlier.astype(BF16), preferred_element_type=F32)
    slots = (rank + 0.5).astype(jnp.int32) + expert * CAP
    dest0 = jnp.sum(jnp.where(expert == first, slots, 0), axis=0, keepdims=True)
    dest1 = jnp.sum(jnp.where(expert == second, slots, 0), axis=0, keepdims=True)
    slot = lax.broadcasted_iota(jnp.int32, (experts * CAP, rows), 0)
    picks = jnp.where((slot == dest0) | (slot == dest1), 1.0, 0.0).astype(BF16)
    out_ref[...] = jnp.dot(picks, normed, preferred_element_type=F32).astype(BF16)


def dispatch(place, ids, tokens, experts):
    return pl.pallas_call(
        functools.partial(dispatch_kernel, experts),
        out_shape=jax.ShapeDtypeStruct((experts * CAP, 256), BF16),
        in_specs=[SMEM, VMEM, VMEM],
        out_specs=VMEM,
        name="dispatch",
        cost_estimate=pl.CostEstimate(flops=2_000_000_000, bytes_accessed=1200000, transcendentals=0),
    )(place, ids, tokens)


def plan_kernel(experts, ids_ref, logits_ref, out_ref):
    rows = ids_ref.shape[0]
    first, second = ids_ref[:, 0:1], ids_ref[:, 1:2]
    expert = lax.broadcasted_iota(jnp.int32, (rows, 128), 1)
    chosen = jnp.where((expert == first) | (expert == second), 1.0, 0.0)
    earlier = jnp.where(
        lax.broadcasted_iota(jnp.int32, (rows, rows), 1)
        < lax.broadcasted_iota(jnp.int32, (rows, rows), 0),
        1.0,
        0.0,
    )
    rank = jnp.dot(earlier.astype(BF16), chosen.astype(BF16), preferred_element_type=F32)
    slots = rank + (expert * CAP).astype(F32)
    dest0 = jnp.sum(jnp.where(expert == first, slots, 0.0), axis=1, keepdims=True)
    dest1 = jnp.sum(jnp.where(expert == second, slots, 0.0), axis=1, keepdims=True)
    weight0 = jax.nn.sigmoid(logits_ref[:, 0:1] - logits_ref[:, 1:2])
    weight1 = jax.nn.sigmoid(logits_ref[:, 1:2] - logits_ref[:, 0:1])
    column = lax.broadcasted_iota(jnp.int32, (rows, 128), 1)
    out_ref[...] = jnp.where(
        column == 0,
        dest0,
        jnp.where(column == 1, dest1, jnp.where(column == 2, weight0, weight1)),
    )


def plan(ids, logits, experts):
    return pl.pallas_call(
        functools.partial(plan_kernel, experts),
        out_shape=jax.ShapeDtypeStruct((ids.shape[0], 128), F32),
        in_specs=[VMEM, VMEM],
        out_specs=VMEM,
        name="plan",
        cost_estimate=pl.CostEstimate(flops=1_000_000_000, bytes_accessed=200000, transcendentals=0),
    )(ids, logits)


def expert_kernel(place, *refs):
    rows_in, refs = refs[:10], refs[10:]
    weights_in, refs = refs[0], refs[1:]
    gate_out, up_out, down_out, hidden_ref, send_ref = refs[:5]
    rows, gate, up, down, in_sem, out_sem = refs[5:]
    x, c = place[0], place[1]
    half = rows.shape[0] // 2
    copies = []
    for k, matrix in enumerate((gate, up, down)):
        for y in range(8):
            copies.append(
                pltpu.make_async_copy(
                    weights_in.at[y, :, k], matrix.at[:, y], in_sem.at[k * 8 + y]
                )
            )
    row_copies = []
    for core in range(2):
        own, left, right, far_a, far_b = rows_in[core * 5 : core * 5 + 5]
        side = c if core == 0 else 1 - c
        for piece, dx, low, size in (
            (own, 0, 0, 2 * half),
            (left, 3, 0, 2 * half),
            (right, 1, 0, 2 * half),
            (far_a, 2, 0, half),
            (far_b, 2, half, half),
        ):
            block = pl.multiple_of((side * 4 + lax.rem(x + dx, 4)) * 256, 256)
            row_copies.append(
                pltpu.make_async_copy(
                    piece,
                    rows.at[pl.ds(low, size), pl.ds(block, 256)],
                    in_sem.at[24 + len(row_copies)],
                )
            )
    for copy in copies[:16] + row_copies + copies[16:]:
        copy.start()
    for copy in copies[:16]:
        copy.wait()
    outs = [
        pltpu.make_async_copy(gate, gate_out, out_sem.at[0]),
        pltpu.make_async_copy(up, up_out, out_sem.at[1]),
        pltpu.make_async_copy(down, down_out, out_sem.at[2]),
    ]
    outs[0].start()
    outs[1].start()
    for copy in row_copies:
        copy.wait()
    gate_matrix = gate[...].reshape(2048, 256)
    up_matrix = up[...].reshape(2048, 256)
    tile = 128

    def first(i, carry):
        low = pl.multiple_of(i * tile, tile)
        piece = rows[pl.ds(low, tile), :]
        gate_act = jnp.dot(piece, gate_matrix, preferred_element_type=F32)
        up_act = jnp.dot(piece, up_matrix, preferred_element_type=F32)
        hidden = gate_act / (1.0 + jnp.exp(-gate_act)) * up_act
        hidden_ref[pl.ds(low, tile), :] = hidden.astype(BF16)
        return carry

    lax.fori_loop(0, rows.shape[0] // tile, first, 0)
    for copy in copies[16:]:
        copy.wait()
    outs[2].start()

    def second(b, carry):
        part = down[pl.ds((1 - c) * 4 + b, 1)].reshape(256, 256)
        send_ref[b] = lax.dot_general(
            hidden_ref[...], part, (((1,), (1,)), ((), ())), preferred_element_type=F32
        ).astype(BF16)
        return carry

    lax.fori_loop(0, 4, second, 0)
    for copy in outs:
        copy.wait()


def expert(place, rows_in, weights):
    count = rows_in[0].shape[0]
    matrix = jax.ShapeDtypeStruct((8, 8, 32, 256), BF16)
    return pl.pallas_call(
        expert_kernel,
        out_shape=(
            matrix,
            matrix,
            matrix,
            jax.ShapeDtypeStruct((count, 256), BF16),
            jax.ShapeDtypeStruct((4, count, 256), BF16),
        ),
        in_specs=[SMEM] + [ANY] * 11,
        out_specs=(ANY, ANY, ANY, VMEM, VMEM),
        scratch_shapes=[
            pltpu.VMEM((count, 2048), BF16),
            pltpu.VMEM((8, 8, 32, 256), BF16),
            pltpu.VMEM((8, 8, 32, 256), BF16),
            pltpu.VMEM((8, 8, 32, 256), BF16),
            pltpu.SemaphoreType.DMA((34,)),
            pltpu.SemaphoreType.DMA((3,)),
        ],
        compiler_params=pltpu.CompilerParams(vmem_limit_bytes=32 * 1024 * 1024),
        name="expert",
        cost_estimate=pl.CostEstimate(flops=8_000_000_000, bytes_accessed=12000000, transcendentals=0),
    )(place, *rows_in, weights)


def own_half_kernel(place, hidden_ref, down_ref, out_ref):
    def step(b, carry):
        part = down_ref[pl.ds(place[1] * 4 + b, 1)].reshape(256, 256)
        out_ref[b] = lax.dot_general(
            hidden_ref[...], part, (((1,), (1,)), ((), ())), preferred_element_type=F32
        ).astype(BF16)
        return carry

    lax.fori_loop(0, 4, step, 0)


def own_half(place, hidden, down):
    return pl.pallas_call(
        own_half_kernel,
        out_shape=jax.ShapeDtypeStruct((4,) + hidden.shape, BF16),
        in_specs=[SMEM, VMEM, VMEM],
        out_specs=VMEM,
        name="own_half",
        cost_estimate=pl.CostEstimate(flops=3_000_000_000, bytes_accessed=3000000, transcendentals=0),
    )(place, hidden, down)


def combine_kernel(plan_ref, back_ref, out_ref):
    rows, slots = plan_ref.shape[0], back_ref.shape[0]
    slot = lax.broadcasted_iota(jnp.int32, (rows, slots), 1)
    back = back_ref[...]
    picked = []
    for k in range(2):
        dest = (plan_ref[:, k : k + 1] + 0.5).astype(jnp.int32)
        onehot = jnp.where(slot == dest, 1.0, 0.0).astype(BF16)
        picked.append(jnp.dot(onehot, back, preferred_element_type=F32))
    out_ref[...] = (plan_ref[:, 2:3] * picked[0] + plan_ref[:, 3:4] * picked[1]).astype(BF16)


def combine(planned, back):
    return pl.pallas_call(
        combine_kernel,
        out_shape=jax.ShapeDtypeStruct((planned.shape[0], 256), BF16),
        in_specs=[VMEM, VMEM],
        out_specs=VMEM,
        name="combine",
        cost_estimate=pl.CostEstimate(flops=1_000_000_000, bytes_accessed=600000, transcendentals=0),
    )(planned, back)


def assemble_kernel(place, own_ref, other_ref, out_ref):
    x, c = place[0], place[1]
    for side, ref in ((c, own_ref), (1 - c, other_ref)):
        for k in range(4):
            block = pl.multiple_of((side * 4 + lax.rem(x + 4 - k, 4)) * 256, 256)
            out_ref[:, pl.ds(block, 256)] = ref[k]


def assemble(place, own, other):
    rows = own.shape[1]
    return pl.pallas_call(
        assemble_kernel,
        out_shape=jax.ShapeDtypeStruct((rows, 2048), BF16),
        in_specs=[SMEM, VMEM, VMEM],
        out_specs=VMEM,
        name="assemble",
        cost_estimate=pl.CostEstimate(flops=100_000_000, bytes_accessed=1600000, transcendentals=0),
    )(place, own, other)


def body(tokens, route_ids, route_logits, norm_gain, gate_weight, up_weight, down_weight):
    experts = gate_weight.shape[0]
    x, c = lax.axis_index("x"), lax.axis_index("c")
    place = jnp.stack([x, c]).astype(jnp.int32)
    scaled_gain = norm_gain[None, :, None]
    packed = jnp.stack(
        [
            (scaled_gain * gate_weight).astype(BF16),
            (scaled_gain * up_weight).astype(BF16),
            down_weight.astype(BF16),
        ],
        axis=1,
    )
    slab = lax.all_to_all(packed, "z", split_axis=0, concat_axis=0, tiled=True)
    weights = lax.all_gather(slab, "y", axis=0, tiled=False)

    sent = dispatch(place, route_ids.T, tokens, experts).reshape(experts, CAP, 256)
    arrived = lax.all_to_all(sent, "z", split_axis=0, concat_axis=0, tiled=True)
    arrived = arrived.reshape(-1, 256)
    half = arrived.shape[0] // 2
    left = shift(arrived, "x", 1)
    right = shift(arrived, "x", -1)
    far_a = shift(left[:half], "x", 1)
    far_b = shift(right[half:], "x", -1)
    mine = [arrived, left, right, far_a, far_b]
    theirs = [swap(piece) for piece in mine]

    gate_new, up_new, down_new, hidden, send = expert(place, mine + theirs, weights)
    received = swap(send)
    own = own_half(place, hidden, down_new.reshape(8, 256, 256))

    def block(dx, low, size):
        at = (lax.rem(x + dx, 4), low, 0)
        cut = (1, size, 256)
        return (
            lax.dynamic_slice(own, at, cut)[0].astype(F32)
            + lax.dynamic_slice(received, at, cut)[0].astype(F32)
        )

    from_left = shift(block(2, 0, half).astype(BF16), "x", 1)
    from_right = shift(block(2, half, half).astype(BF16), "x", -1)
    to_right = jnp.concatenate(
        [block(1, 0, half) + from_left.astype(F32), block(1, half, half)], axis=0
    ).astype(BF16)
    to_left = jnp.concatenate(
        [block(3, 0, half), block(3, half, half) + from_right.astype(F32)], axis=0
    ).astype(BF16)
    share = (
        block(0, 0, 2 * half)
        + shift(to_right, "x", 1).astype(F32)
        + shift(to_left, "x", -1).astype(F32)
    ).astype(BF16)
    back = lax.all_to_all(
        share.reshape(experts, CAP, 256), "z", split_axis=0, concat_axis=0, tiled=True
    ).reshape(-1, 256)
    mixed = combine(plan(route_ids, route_logits, experts), back)
    ring = jnp.stack([mixed, shift(mixed, "x", 1), shift(mixed, "x", 2), shift(mixed, "x", 3)])
    mixed = assemble(place, ring, swap(ring))
    shape = (1, 2048, 256)
    return (mixed, gate_new.reshape(shape), up_new.reshape(shape), down_new.reshape(shape))


def solution(mesh):
    grid = Mesh(mesh.devices.reshape(8, 8, 4, 2), ("z", "y", "x", "c"))
    fs, tp = ("z", "y"), ("x", "c")
    return jax.shard_map(
        body,
        mesh=grid,
        in_specs=(
            P(fs, None),
            P(fs, None),
            P(fs, None),
            P(fs),
            P(None, fs, tp),
            P(None, fs, tp),
            P(None, fs, tp),
        ),
        out_specs=(P(fs, None), P(fs, None, tp), P(fs, None, tp), P(fs, None, tp)),
        check_vma=False,
    )
```

```python
import functools

import jax
import jax.numpy as jnp
from jax import lax
from jax.experimental import pallas as pl
from jax.experimental.pallas import tpu as pltpu
from jax.sharding import Mesh
from jax.sharding import PartitionSpec as P

CAP = 96
BF16 = jnp.bfloat16
F32 = jnp.float32
VMEM = pl.BlockSpec(memory_space=pltpu.VMEM)
SMEM = pl.BlockSpec(memory_space=pltpu.SMEM)


def shift(value, axis, by):
    size = lax.axis_size(axis)
    return lax.ppermute(value, axis, [(i, (i + by) % size) for i in range(size)])


def swap(value):
    return lax.ppermute(value, "c", [(0, 1), (1, 0)])


def dispatch_kernel(experts, place, ids_ref, tokens_ref, out_ref):
    rows = tokens_ref.shape[0]
    values = tokens_ref[...].astype(F32)
    center = jnp.mean(values, axis=1, keepdims=True)
    spread = jnp.mean(jnp.square(values - center), axis=1, keepdims=True)
    start = pl.multiple_of((place[1] * 4 + place[0]) * 256, 256)
    own = tokens_ref[:, pl.ds(start, 256)].astype(F32)
    normed = ((own - center) * lax.rsqrt(spread + 1e-06)).astype(BF16)
    first, second = ids_ref[0:1, :], ids_ref[1:2, :]
    expert = lax.broadcasted_iota(jnp.int32, (experts, rows), 0)
    chosen = jnp.where((expert == first) | (expert == second), 1.0, 0.0)
    earlier = jnp.where(
        lax.broadcasted_iota(jnp.int32, (rows, rows), 0)
        < lax.broadcasted_iota(jnp.int32, (rows, rows), 1),
        1.0,
        0.0,
    )
    rank = jnp.dot(chosen.astype(BF16), earlier.astype(BF16), preferred_element_type=F32)
    slots = (rank + 0.5).astype(jnp.int32) + expert * CAP
    dest0 = jnp.sum(jnp.where(expert == first, slots, 0), axis=0, keepdims=True)
    dest1 = jnp.sum(jnp.where(expert == second, slots, 0), axis=0, keepdims=True)
    slot = lax.broadcasted_iota(jnp.int32, (experts * CAP, rows), 0)
    picks = jnp.where((slot == dest0) | (slot == dest1), 1.0, 0.0).astype(BF16)
    out_ref[...] = jnp.dot(picks, normed, preferred_element_type=F32).astype(BF16)


def dispatch(place, ids, tokens, experts):
    return pl.pallas_call(
        functools.partial(dispatch_kernel, experts),
        out_shape=jax.ShapeDtypeStruct((experts * CAP, 256), BF16),
        in_specs=[SMEM, VMEM, VMEM],
        out_specs=VMEM,
        compiler_params=pltpu.CompilerParams(vmem_limit_bytes=12 * 1024 * 1024),
        name="dispatch",
        cost_estimate=pl.CostEstimate(flops=2_000_000_000, bytes_accessed=1200000, transcendentals=0),
    )(place, ids, tokens)


def plan_kernel(experts, ids_ref, logits_ref, out_ref):
    rows = ids_ref.shape[0]
    first, second = ids_ref[:, 0:1], ids_ref[:, 1:2]
    expert = lax.broadcasted_iota(jnp.int32, (rows, 128), 1)
    chosen = jnp.where((expert == first) | (expert == second), 1.0, 0.0)
    earlier = jnp.where(
        lax.broadcasted_iota(jnp.int32, (rows, rows), 1)
        < lax.broadcasted_iota(jnp.int32, (rows, rows), 0),
        1.0,
        0.0,
    )
    rank = jnp.dot(earlier.astype(BF16), chosen.astype(BF16), preferred_element_type=F32)
    slots = rank + (expert * CAP).astype(F32)
    dest0 = jnp.sum(jnp.where(expert == first, slots, 0.0), axis=1, keepdims=True)
    dest1 = jnp.sum(jnp.where(expert == second, slots, 0.0), axis=1, keepdims=True)
    weight0 = jax.nn.sigmoid(logits_ref[:, 0:1] - logits_ref[:, 1:2])
    weight1 = jax.nn.sigmoid(logits_ref[:, 1:2] - logits_ref[:, 0:1])
    column = lax.broadcasted_iota(jnp.int32, (rows, 128), 1)
    out_ref[...] = jnp.where(
        column == 0,
        dest0,
        jnp.where(column == 1, dest1, jnp.where(column == 2, weight0, weight1)),
    )


def plan(ids, logits, experts):
    return pl.pallas_call(
        functools.partial(plan_kernel, experts),
        out_shape=jax.ShapeDtypeStruct((ids.shape[0], 128), F32),
        in_specs=[VMEM, VMEM],
        out_specs=VMEM,
        compiler_params=pltpu.CompilerParams(vmem_limit_bytes=4 * 1024 * 1024),
        name="plan",
        cost_estimate=pl.CostEstimate(flops=1_000_000_000, bytes_accessed=200000, transcendentals=0),
    )(ids, logits)


def expert_kernel(place, *refs):
    sides, slabs = (refs[:5], refs[5:10]), refs[10:19]
    gate_out, up_out, down_out, hidden_ref, send_ref, rows = refs[19:]
    x, c, y = place[0], place[1], place[2]
    half = rows.shape[0] // 2
    for slab, dy, low, size in (
        (slabs[0], 0, 0, 8),
        (slabs[1], 7, 0, 8),
        (slabs[2], 1, 0, 8),
        (slabs[3], 6, 0, 8),
        (slabs[4], 2, 0, 8),
        (slabs[5], 5, 0, 8),
        (slabs[6], 3, 0, 8),
        (slabs[7], 4, 0, 4),
        (slabs[8], 4, 4, 4),
    ):
        at = lax.rem(y + dy, 8)
        for k, out in enumerate((gate_out, up_out, down_out)):
            out[pl.ds(low, size), pl.ds(at, 1)] = slab[:, k : k + 1]
    for core in range(2):
        side = c if core == 0 else 1 - c
        own, left, right, far_a, far_b = sides[core]
        for piece, dx, low, size in (
            (own, 0, 0, 2 * half),
            (left, 3, 0, 2 * half),
            (right, 1, 0, 2 * half),
            (far_a, 2, 0, half),
            (far_b, 2, half, half),
        ):
            block = pl.multiple_of((side * 4 + lax.rem(x + dx, 4)) * 256, 256)
            rows[low : low + size, pl.ds(block, 256)] = piece[...]
    tile = 128

    def first(i, carry):
        low = pl.multiple_of(i * tile, tile)
        piece = rows[pl.ds(low, tile), :]
        gate_act = jnp.dot(piece, gate_out[...].reshape(2048, 256), preferred_element_type=F32)
        up_act = jnp.dot(piece, up_out[...].reshape(2048, 256), preferred_element_type=F32)
        hidden = gate_act / (1.0 + jnp.exp(-gate_act)) * up_act
        hidden_ref[pl.ds(low, tile), :] = hidden.astype(BF16)
        return carry

    lax.fori_loop(0, rows.shape[0] // tile, first, 0)

    def second(b, carry):
        part = down_out[pl.ds((1 - c) * 4 + b, 1)].reshape(256, 256)
        send_ref[b] = lax.dot_general(
            hidden_ref[...], part, (((1,), (1,)), ((), ())), preferred_element_type=F32
        ).astype(BF16)
        return carry

    lax.fori_loop(0, 4, second, 0)


def expert(place, mine, theirs, slabs):
    count = mine[0].shape[0]
    matrix = jax.ShapeDtypeStruct((8, 8, 32, 256), BF16)
    return pl.pallas_call(
        expert_kernel,
        out_shape=(
            matrix,
            matrix,
            matrix,
            jax.ShapeDtypeStruct((count, 256), BF16),
            jax.ShapeDtypeStruct((4, count, 256), BF16),
        ),
        in_specs=[SMEM] + [VMEM] * 19,
        out_specs=(VMEM,) * 5,
        scratch_shapes=[pltpu.VMEM((count, 2048), BF16)],
        compiler_params=pltpu.CompilerParams(vmem_limit_bytes=24 * 1024 * 1024),
        name="expert",
        cost_estimate=pl.CostEstimate(flops=8_000_000_000, bytes_accessed=12000000, transcendentals=0),
    )(place, *mine, *theirs, *slabs)


def own_half_kernel(place, hidden_ref, down_ref, out_ref):
    def step(b, carry):
        part = down_ref[pl.ds(place[1] * 4 + b, 1)].reshape(256, 256)
        out_ref[b] = lax.dot_general(
            hidden_ref[...], part, (((1,), (1,)), ((), ())), preferred_element_type=F32
        ).astype(BF16)
        return carry

    lax.fori_loop(0, 4, step, 0)


def own_half(place, hidden, down):
    return pl.pallas_call(
        own_half_kernel,
        out_shape=jax.ShapeDtypeStruct((4,) + hidden.shape, BF16),
        in_specs=[SMEM, VMEM, VMEM],
        out_specs=VMEM,
        compiler_params=pltpu.CompilerParams(vmem_limit_bytes=8 * 1024 * 1024),
        name="own_half",
        cost_estimate=pl.CostEstimate(flops=3_000_000_000, bytes_accessed=3000000, transcendentals=0),
    )(place, hidden, down)


def combine_kernel(plan_ref, back_ref, out_ref):
    rows, slots = plan_ref.shape[0], back_ref.shape[0]
    slot = lax.broadcasted_iota(jnp.int32, (rows, slots), 1)
    back = back_ref[...]
    picked = []
    for k in range(2):
        dest = (plan_ref[:, k : k + 1] + 0.5).astype(jnp.int32)
        onehot = jnp.where(slot == dest, 1.0, 0.0).astype(BF16)
        picked.append(jnp.dot(onehot, back, preferred_element_type=F32))
    out_ref[...] = (plan_ref[:, 2:3] * picked[0] + plan_ref[:, 3:4] * picked[1]).astype(BF16)


def combine(planned, back):
    return pl.pallas_call(
        combine_kernel,
        out_shape=jax.ShapeDtypeStruct((planned.shape[0], 256), BF16),
        in_specs=[VMEM, VMEM],
        out_specs=VMEM,
        compiler_params=pltpu.CompilerParams(vmem_limit_bytes=6 * 1024 * 1024),
        name="combine",
        cost_estimate=pl.CostEstimate(flops=1_000_000_000, bytes_accessed=600000, transcendentals=0),
    )(planned, back)


def assemble_kernel(ring_ref, out_ref):
    for x in range(4):
        for c in range(2):
            low = (c * 4 + x) * 256
            out_ref[:, low : low + 256] = ring_ref[2 * x + c]


def assemble(ring):
    rows = ring.shape[1]
    return pl.pallas_call(
        assemble_kernel,
        out_shape=jax.ShapeDtypeStruct((rows, 2048), BF16),
        in_specs=[VMEM],
        out_specs=VMEM,
        compiler_params=pltpu.CompilerParams(vmem_limit_bytes=6 * 1024 * 1024),
        name="assemble",
        cost_estimate=pl.CostEstimate(flops=100_000_000, bytes_accessed=1600000, transcendentals=0),
    )(ring)


def ring_of(value, axis):
    steps = lax.axis_size(axis) // 2
    cut = value.shape[0] // 2
    pieces, left, right = [value], value, value
    for _ in range(steps - 1):
        left, right = shift(left, axis, 1), shift(right, axis, -1)
        pieces += [left, right]
    return pieces + [shift(left[:cut], axis, 1), shift(right[cut:], axis, -1)]


def body(tokens, route_ids, route_logits, norm_gain, gate_weight, up_weight, down_weight):
    experts = gate_weight.shape[0]
    x, c = lax.axis_index("x"), lax.axis_index("c")
    place = jnp.stack([x, c, lax.axis_index("y")]).astype(jnp.int32)
    scaled_gain = norm_gain[None, :, None]
    packed = jnp.stack(
        [
            (scaled_gain * gate_weight).astype(BF16),
            (scaled_gain * up_weight).astype(BF16),
            down_weight.astype(BF16),
        ],
        axis=1,
    )
    slab = lax.all_to_all(packed, "z", split_axis=0, concat_axis=0, tiled=True)
    slabs = ring_of(slab, "y")

    sent = dispatch(place, route_ids.T, tokens, experts).reshape(experts, CAP, 256)
    arrived = lax.all_to_all(sent, "z", split_axis=0, concat_axis=0, tiled=True)
    mine = ring_of(arrived.reshape(-1, 256), "x")
    theirs = [swap(piece) for piece in mine]

    gate_new, up_new, down_new, hidden, send = expert(place, mine, theirs, slabs)
    received = swap(send)
    own = own_half(place, hidden, down_new.reshape(8, 256, 256))
    pairs = (own.astype(F32) + received.astype(F32)).astype(BF16)
    parts = lax.all_to_all(pairs, "x", split_axis=0, concat_axis=0, tiled=True)
    share = jnp.sum(parts.astype(F32), axis=0).astype(BF16)
    back = lax.all_to_all(
        share.reshape(experts, CAP, 256), "z", split_axis=0, concat_axis=0, tiled=True
    ).reshape(-1, 256)
    mixed = combine(plan(route_ids, route_logits, experts), back)
    ring = lax.all_gather(mixed, ("x", "c"), axis=0, tiled=False)
    mixed = assemble(ring)
    shape = (1, 2048, 256)
    return (mixed, gate_new.reshape(shape), up_new.reshape(shape), down_new.reshape(shape))


def solution(mesh):
    grid = Mesh(mesh.devices.reshape(8, 8, 4, 2), ("z", "y", "x", "c"))
    fs, tp = ("z", "y"), ("x", "c")
    return jax.shard_map(
        body,
        mesh=grid,
        in_specs=(
            P(fs, None),
            P(fs, None),
            P(fs, None),
            P(fs),
            P(None, fs, tp),
            P(None, fs, tp),
            P(None, fs, tp),
        ),
        out_specs=(P(fs, None), P(fs, None, tp), P(fs, None, tp), P(fs, None, tp)),
        check_vma=False,
    )
```

```python
import functools

import jax
import jax.numpy as jnp
from jax import lax
from jax.experimental import pallas as pl
from jax.experimental.pallas import tpu as pltpu
from jax.sharding import Mesh
from jax.sharding import PartitionSpec as P


CAP = 96
BF16 = jnp.bfloat16
F32 = jnp.float32
VMEM = pl.BlockSpec(memory_space=pltpu.VMEM)
SMEM = pl.BlockSpec(memory_space=pltpu.SMEM)


def shift(value, axis, by):
    size = lax.axis_size(axis)
    return lax.ppermute(value, axis, [(i, (i + by) % size) for i in range(size)])


def swap(value):
    return lax.ppermute(value, "c", [(0, 1), (1, 0)])


def dispatch_kernel(experts, place, ids_ref, tokens_ref, out_ref):
    rows = tokens_ref.shape[0]
    values = tokens_ref[...].astype(F32)
    center = jnp.mean(values, axis=1, keepdims=True)
    spread = jnp.mean(jnp.square(values - center), axis=1, keepdims=True)
    start = pl.multiple_of((place[1] * 4 + place[0]) * 256, 256)
    own = tokens_ref[:, pl.ds(start, 256)].astype(F32)
    normed = ((own - center) * lax.rsqrt(spread + 1e-06)).astype(BF16)
    first, second = ids_ref[0:1, :], ids_ref[1:2, :]
    expert = lax.broadcasted_iota(jnp.int32, (experts, rows), 0)
    chosen = jnp.where((expert == first) | (expert == second), 1.0, 0.0)
    earlier = jnp.where(
        lax.broadcasted_iota(jnp.int32, (rows, rows), 0)
        < lax.broadcasted_iota(jnp.int32, (rows, rows), 1),
        1.0,
        0.0,
    )
    rank = jnp.dot(chosen.astype(BF16), earlier.astype(BF16), preferred_element_type=F32)
    slots = (rank + 0.5).astype(jnp.int32) + expert * CAP
    dest0 = jnp.sum(jnp.where(expert == first, slots, 0), axis=0, keepdims=True)
    dest1 = jnp.sum(jnp.where(expert == second, slots, 0), axis=0, keepdims=True)
    slot = lax.broadcasted_iota(jnp.int32, (experts * CAP, rows), 0)
    picks = jnp.where((slot == dest0) | (slot == dest1), 1.0, 0.0).astype(BF16)
    out_ref[...] = jnp.dot(picks, normed, preferred_element_type=F32).astype(BF16)


def dispatch(place, ids, tokens, experts):
    return pl.pallas_call(
        functools.partial(dispatch_kernel, experts),
        out_shape=jax.ShapeDtypeStruct((experts * CAP, 256), BF16),
        in_specs=[SMEM, VMEM, VMEM],
        out_specs=VMEM,
        compiler_params=pltpu.CompilerParams(vmem_limit_bytes=12 * 1024 * 1024),
        name="dispatch",
        cost_estimate=pl.CostEstimate(flops=2_000_000_000, bytes_accessed=1200000, transcendentals=0),
    )(place, ids, tokens)


def plan_kernel(ids_ref, logits_ref, out_ref):
    rows = ids_ref.shape[0]
    first, second = ids_ref[:, 0:1], ids_ref[:, 1:2]
    expert = lax.broadcasted_iota(jnp.int32, (rows, 128), 1)
    chosen = jnp.where((expert == first) | (expert == second), 1.0, 0.0)
    earlier = jnp.where(
        lax.broadcasted_iota(jnp.int32, (rows, rows), 1)
        < lax.broadcasted_iota(jnp.int32, (rows, rows), 0),
        1.0,
        0.0,
    )
    rank = jnp.dot(earlier.astype(BF16), chosen.astype(BF16), preferred_element_type=F32)
    slots = rank + (expert * CAP).astype(F32)
    dest0 = jnp.sum(jnp.where(expert == first, slots, 0.0), axis=1, keepdims=True)
    dest1 = jnp.sum(jnp.where(expert == second, slots, 0.0), axis=1, keepdims=True)
    weight0 = jax.nn.sigmoid(logits_ref[:, 0:1] - logits_ref[:, 1:2])
    weight1 = jax.nn.sigmoid(logits_ref[:, 1:2] - logits_ref[:, 0:1])
    column = lax.broadcasted_iota(jnp.int32, (rows, 128), 1)
    out_ref[...] = jnp.where(
        column == 0,
        dest0,
        jnp.where(column == 1, dest1, jnp.where(column == 2, weight0, weight1)),
    )


def plan(ids, logits):
    return pl.pallas_call(
        plan_kernel,
        out_shape=jax.ShapeDtypeStruct((ids.shape[0], 128), F32),
        in_specs=[VMEM, VMEM],
        out_specs=VMEM,
        compiler_params=pltpu.CompilerParams(vmem_limit_bytes=4 * 1024 * 1024),
        name="plan",
        cost_estimate=pl.CostEstimate(flops=1_000_000_000, bytes_accessed=200000, transcendentals=0),
    )(ids, logits)


def expert_kernel(place, *refs):
    sides, slabs = refs[:2], refs[2:11]
    gate_out, up_out, down_out, hidden_ref, send_ref, rows = refs[11:]
    c, y = place[1], place[2]
    for slab, dy, low, size in (
        (slabs[0], 0, 0, 8),
        (slabs[1], 7, 0, 8),
        (slabs[2], 1, 0, 8),
        (slabs[3], 6, 0, 8),
        (slabs[4], 2, 0, 8),
        (slabs[5], 5, 0, 8),
        (slabs[6], 3, 0, 8),
        (slabs[7], 4, 0, 4),
        (slabs[8], 4, 4, 4),
    ):
        at = lax.rem(y + dy, 8)
        for k, out in enumerate((gate_out, up_out, down_out)):
            out[pl.ds(low, size), pl.ds(at, 1)] = slab[:, k : k + 1]
    for core in range(2):
        side = c if core == 0 else 1 - c
        for x in range(4):
            block = pl.multiple_of((side * 4 + x) * 256, 256)
            rows[:, pl.ds(block, 256)] = sides[core][x]
    tile = 128

    def first(i, carry):
        low = pl.multiple_of(i * tile, tile)
        piece = rows[pl.ds(low, tile), :]
        gate_act = jnp.dot(piece, gate_out[...].reshape(2048, 256), preferred_element_type=F32)
        up_act = jnp.dot(piece, up_out[...].reshape(2048, 256), preferred_element_type=F32)
        hidden = gate_act / (1.0 + jnp.exp(-gate_act)) * up_act
        hidden_ref[pl.ds(low, tile), :] = hidden.astype(BF16)
        return carry

    lax.fori_loop(0, rows.shape[0] // tile, first, 0)

    def second(b, carry):
        part = down_out[pl.ds((1 - c) * 4 + b, 1)].reshape(256, 256)
        send_ref[b] = lax.dot_general(
            hidden_ref[...], part, (((1,), (1,)), ((), ())), preferred_element_type=F32
        ).astype(BF16)
        return carry

    lax.fori_loop(0, 4, second, 0)


def expert(place, mine, theirs, slabs):
    count = mine.shape[1]
    matrix = jax.ShapeDtypeStruct((8, 8, 32, 256), BF16)
    return pl.pallas_call(
        expert_kernel,
        out_shape=(
            matrix,
            matrix,
            matrix,
            jax.ShapeDtypeStruct((count, 256), BF16),
            jax.ShapeDtypeStruct((4, count, 256), BF16),
        ),
        in_specs=[SMEM] + [VMEM] * 11,
        out_specs=(VMEM,) * 5,
        scratch_shapes=[pltpu.VMEM((count, 2048), BF16)],
        compiler_params=pltpu.CompilerParams(vmem_limit_bytes=24 * 1024 * 1024),
        name="expert",
        cost_estimate=pl.CostEstimate(flops=8_000_000_000, bytes_accessed=12000000, transcendentals=0),
    )(place, mine, theirs, *slabs)


def own_half_kernel(place, hidden_ref, down_ref, out_ref):
    def step(b, carry):
        part = down_ref[pl.ds(place[1] * 4 + b, 1)].reshape(256, 256)
        out_ref[b] = lax.dot_general(
            hidden_ref[...], part, (((1,), (1,)), ((), ())), preferred_element_type=F32
        ).astype(BF16)
        return carry

    lax.fori_loop(0, 4, step, 0)


def own_half(place, hidden, down):
    return pl.pallas_call(
        own_half_kernel,
        out_shape=jax.ShapeDtypeStruct((4,) + hidden.shape, BF16),
        in_specs=[SMEM, VMEM, VMEM],
        out_specs=VMEM,
        compiler_params=pltpu.CompilerParams(vmem_limit_bytes=8 * 1024 * 1024),
        name="own_half",
        cost_estimate=pl.CostEstimate(flops=3_000_000_000, bytes_accessed=3000000, transcendentals=0),
    )(place, hidden, down)


def combine_kernel(plan_ref, back_ref, out_ref):
    rows, slots = plan_ref.shape[0], back_ref.shape[0]
    slot = lax.broadcasted_iota(jnp.int32, (rows, slots), 1)
    back = back_ref[...]
    picked = []
    for k in range(2):
        dest = (plan_ref[:, k : k + 1] + 0.5).astype(jnp.int32)
        onehot = jnp.where(slot == dest, 1.0, 0.0).astype(BF16)
        picked.append(jnp.dot(onehot, back, preferred_element_type=F32))
    out_ref[...] = (plan_ref[:, 2:3] * picked[0] + plan_ref[:, 3:4] * picked[1]).astype(BF16)


def combine(planned, back):
    return pl.pallas_call(
        combine_kernel,
        out_shape=jax.ShapeDtypeStruct((planned.shape[0], 256), BF16),
        in_specs=[VMEM, VMEM],
        out_specs=VMEM,
        compiler_params=pltpu.CompilerParams(vmem_limit_bytes=6 * 1024 * 1024),
        name="combine",
        cost_estimate=pl.CostEstimate(flops=1_000_000_000, bytes_accessed=600000, transcendentals=0),
    )(planned, back)


def assemble_kernel(ring_ref, out_ref):
    for x in range(4):
        for c in range(2):
            low = (c * 4 + x) * 256
            out_ref[:, low : low + 256] = ring_ref[2 * x + c]


def assemble(ring):
    rows = ring.shape[1]
    return pl.pallas_call(
        assemble_kernel,
        out_shape=jax.ShapeDtypeStruct((rows, 2048), BF16),
        in_specs=[VMEM],
        out_specs=VMEM,
        compiler_params=pltpu.CompilerParams(vmem_limit_bytes=6 * 1024 * 1024),
        name="assemble",
        cost_estimate=pl.CostEstimate(flops=100_000_000, bytes_accessed=1600000, transcendentals=0),
    )(ring)


def ring_of(value):
    pieces, left, right = [value], value, value
    cut = value.shape[0] // 2
    for hop in range(1, 5):
        if hop == 4:
            left, right = left[:cut], right[cut:]
        left = shift(left, "y", 1)
        right = shift(right, "y", -1)
        pieces += [left, right]
    return pieces


def layer(tokens, route_ids, route_logits, norm_gain, gate_weight, up_weight, down_weight):
    experts = gate_weight.shape[0]
    x, c = lax.axis_index("x"), lax.axis_index("c")
    place = jnp.stack([x, c, lax.axis_index("y")]).astype(jnp.int32)
    scaled_gain = norm_gain[None, :, None]
    packed = jnp.stack(
        [
            (scaled_gain * gate_weight).astype(BF16),
            (scaled_gain * up_weight).astype(BF16),
            down_weight.astype(BF16),
        ],
        axis=1,
    )
    slab = lax.all_to_all(packed, "z", split_axis=0, concat_axis=0, tiled=True)
    slabs = ring_of(slab)

    sent = dispatch(place, route_ids.T, tokens, experts).reshape(experts, CAP, 256)
    arrived = lax.all_to_all(sent, "z", split_axis=0, concat_axis=0, tiled=True)
    arrived = arrived.reshape(1, -1, 256)
    spread = jnp.broadcast_to(arrived, (4,) + arrived.shape[1:])
    mine = lax.all_to_all(spread, "x", split_axis=0, concat_axis=0, tiled=True)
    theirs = swap(mine)

    gate_new, up_new, down_new, hidden, send = expert(place, mine, theirs, slabs)
    received = swap(send)
    own = own_half(place, hidden, down_new.reshape(8, 256, 256))
    pairs = (own.astype(F32) + received.astype(F32)).astype(BF16)
    parts = lax.all_to_all(pairs, "x", split_axis=0, concat_axis=0, tiled=True)
    share = jnp.sum(parts.astype(F32), axis=0).astype(BF16)
    back = lax.all_to_all(
        share.reshape(experts, CAP, 256), "z", split_axis=0, concat_axis=0, tiled=True
    ).reshape(-1, 256)
    mixed = combine(plan(route_ids, route_logits), back)
    ring = lax.all_gather(mixed, ("x", "c"), axis=0, tiled=False)
    mixed = assemble(ring)
    shape = (1, 2048, 256)
    return (mixed, gate_new.reshape(shape), up_new.reshape(shape), down_new.reshape(shape))


def solution(mesh):
    grid = Mesh(mesh.devices.reshape(8, 8, 4, 2), ("z", "y", "x", "c"))
    fs, tp = ("z", "y"), ("x", "c")
    return jax.shard_map(
        layer,
        mesh=grid,
        in_specs=(
            P(fs, None),
            P(fs, None),
            P(fs, None),
            P(fs),
            P(None, fs, tp),
            P(None, fs, tp),
            P(None, fs, tp),
        ),
        out_specs=(P(fs, None), P(fs, None, tp), P(fs, None, tp), P(fs, None, tp)),
        check_vma=False,
    )
```

```python
import functools

import jax
import jax.numpy as jnp
from jax import lax
from jax.experimental import pallas as pl
from jax.experimental.pallas import tpu as pltpu
from jax.sharding import Mesh
from jax.sharding import PartitionSpec as P


CAP = 96
BF16 = jnp.bfloat16
F32 = jnp.float32
VMEM = pl.BlockSpec(memory_space=pltpu.VMEM)
SMEM = pl.BlockSpec(memory_space=pltpu.SMEM)
HBM = pl.BlockSpec(memory_space=pltpu.HBM)


def turn(value, axis, by):
    size = lax.axis_size(axis)
    pairs = [(2 * i, 2 * ((i + by) % size)) for i in range(size)]
    pairs += [(2 * i + 1, 2 * ((i - by) % size) + 1) for i in range(size)]
    return lax.ppermute(value, (axis, "c"), pairs)


def swap(value):
    return lax.ppermute(value, "c", [(0, 1), (1, 0)])


def fold_kernel(gain_ref, gate_ref, up_ref, down_ref, out_ref, gain_buf, buffers, sems):
    copies = [pltpu.make_async_copy(gain_ref, gain_buf, sems.at[3])]
    for k, ref in enumerate((gate_ref, up_ref, down_ref)):
        copies.append(pltpu.make_async_copy(ref, buffers.at[k], sems.at[k]))
    for copy in copies:
        copy.start()
    for copy in copies[:2]:
        copy.wait()
    size = gain_ref.shape[1]
    row = lax.broadcasted_iota(jnp.int32, (size, size), 0)
    column = lax.broadcasted_iota(jnp.int32, (size, size), 1)
    gain = jnp.sum(jnp.where(row == column, gain_buf[...], 0.0), axis=1, keepdims=True)
    for e in range(out_ref.shape[0]):
        out_ref[e, 0] = (gain * buffers[0, e]).astype(BF16)
    copies[2].wait()
    for e in range(out_ref.shape[0]):
        out_ref[e, 1] = (gain * buffers[1, e]).astype(BF16)
    copies[3].wait()
    for e in range(out_ref.shape[0]):
        out_ref[e, 2] = buffers[2, e].astype(BF16)


def fold(gain, gate, up, down):
    experts, rows, columns = gate.shape
    return pl.pallas_call(
        fold_kernel,
        out_shape=jax.ShapeDtypeStruct((experts, 3, rows, columns), BF16),
        in_specs=[HBM] * 4,
        out_specs=VMEM,
        scratch_shapes=[
            pltpu.VMEM((1, rows), F32),
            pltpu.VMEM((3, experts, rows, columns), F32),
            pltpu.SemaphoreType.DMA((4,)),
        ],
        name="fold",
        cost_estimate=pl.CostEstimate(flops=500_000_000, bytes_accessed=1200000, transcendentals=0),
    )(gain.reshape(1, rows), gate, up, down)


def dispatch_kernel(experts, place, ids_ref, tokens_ref, out_ref):
    rows = tokens_ref.shape[0]
    values = tokens_ref[...].astype(F32)
    center = jnp.mean(values, axis=1, keepdims=True)
    spread = jnp.mean(jnp.square(values - center), axis=1, keepdims=True)
    start = pl.multiple_of((place[1] * 4 + place[0]) * 256, 256)
    own = tokens_ref[:, pl.ds(start, 256)].astype(F32)
    normed = ((own - center) * lax.rsqrt(spread + 1e-06)).astype(BF16)
    first, second = ids_ref[0:1, :], ids_ref[1:2, :]
    expert = lax.broadcasted_iota(jnp.int32, (experts, rows), 0)
    chosen = jnp.where((expert == first) | (expert == second), 1.0, 0.0)
    earlier = jnp.where(
        lax.broadcasted_iota(jnp.int32, (rows, rows), 0)
        < lax.broadcasted_iota(jnp.int32, (rows, rows), 1),
        1.0,
        0.0,
    )
    rank = jnp.dot(chosen.astype(BF16), earlier.astype(BF16), preferred_element_type=F32)
    slots = (rank + 0.5).astype(jnp.int32) + expert * CAP
    dest0 = jnp.sum(jnp.where(expert == first, slots, 0), axis=0, keepdims=True)
    dest1 = jnp.sum(jnp.where(expert == second, slots, 0), axis=0, keepdims=True)
    slot = lax.broadcasted_iota(jnp.int32, (experts * CAP, rows), 0)
    picks = jnp.where((slot == dest0) | (slot == dest1), 1.0, 0.0).astype(BF16)
    out_ref[...] = jnp.dot(picks, normed, preferred_element_type=F32).astype(BF16)


def dispatch(place, ids, tokens, experts):
    return pl.pallas_call(
        functools.partial(dispatch_kernel, experts),
        out_shape=jax.ShapeDtypeStruct((experts * CAP, 256), BF16),
        in_specs=[SMEM, VMEM, VMEM],
        out_specs=VMEM,
        compiler_params=pltpu.CompilerParams(vmem_limit_bytes=12 * 1024 * 1024),
        name="dispatch",
        cost_estimate=pl.CostEstimate(flops=2_000_000_000, bytes_accessed=1200000, transcendentals=0),
    )(place, ids, tokens)


def plan_kernel(ids_ref, logits_ref, out_ref):
    rows = ids_ref.shape[0]
    first, second = ids_ref[:, 0:1], ids_ref[:, 1:2]
    expert = lax.broadcasted_iota(jnp.int32, (rows, 128), 1)
    chosen = jnp.where((expert == first) | (expert == second), 1.0, 0.0)
    earlier = jnp.where(
        lax.broadcasted_iota(jnp.int32, (rows, rows), 1)
        < lax.broadcasted_iota(jnp.int32, (rows, rows), 0),
        1.0,
        0.0,
    )
    rank = jnp.dot(earlier.astype(BF16), chosen.astype(BF16), preferred_element_type=F32)
    slots = rank + (expert * CAP).astype(F32)
    dest0 = jnp.sum(jnp.where(expert == first, slots, 0.0), axis=1, keepdims=True)
    dest1 = jnp.sum(jnp.where(expert == second, slots, 0.0), axis=1, keepdims=True)
    weight0 = jax.nn.sigmoid(logits_ref[:, 0:1] - logits_ref[:, 1:2])
    weight1 = jax.nn.sigmoid(logits_ref[:, 1:2] - logits_ref[:, 0:1])
    column = lax.broadcasted_iota(jnp.int32, (rows, 128), 1)
    out_ref[...] = jnp.where(
        column == 0,
        dest0,
        jnp.where(column == 1, dest1, jnp.where(column == 2, weight0, weight1)),
    )


def plan(ids, logits):
    return pl.pallas_call(
        plan_kernel,
        out_shape=jax.ShapeDtypeStruct((ids.shape[0], 128), F32),
        in_specs=[VMEM, VMEM],
        out_specs=VMEM,
        compiler_params=pltpu.CompilerParams(vmem_limit_bytes=4 * 1024 * 1024),
        name="plan",
        cost_estimate=pl.CostEstimate(flops=1_000_000_000, bytes_accessed=200000, transcendentals=0),
    )(ids, logits)


def lowered(hidden, down, x, side, out, which):
    ahead = 1 - 2 * side
    offsets = (0, ahead, 2, -ahead)
    for j, k in enumerate(which):
        part = down[pl.ds(side * 4 + lax.rem(x + 4 + offsets[k], 4), 1)].reshape(256, 256)
        out[j] = lax.dot_general(
            hidden[...], part, (((1,), (1,)), ((), ())), preferred_element_type=F32
        ).astype(BF16)


def expert_kernel(place, *refs):
    sides, slabs = refs[:2], refs[2:10]
    gate_out, up_out, down_out, down_ref, hidden_ref, send_ref, rows = refs[10:]
    x, c, y = place[0], place[1], place[2]
    ahead = 1 - 2 * c
    for slab, hops in zip(slabs, (0, -1, 1, -2, 2, -3, 3, -4)):
        at = lax.rem(y + 8 + hops * ahead, 8)
        for k, out in enumerate((gate_out, up_out, down_out)):
            out[:, pl.ds(at, 1)] = slab[:, k : k + 1]
    for core in range(2):
        side = c if core == 0 else 1 - c
        for source in range(4):
            block = pl.multiple_of((side * 4 + source) * 256, 256)
            rows[:, pl.ds(block, 256)] = sides[core][source]
    tile = 128

    def first(i, carry):
        low = pl.multiple_of(i * tile, tile)
        piece = rows[pl.ds(low, tile), :]
        gate_act = jnp.dot(piece, gate_out[...].reshape(2048, 256), preferred_element_type=F32)
        up_act = jnp.dot(piece, up_out[...].reshape(2048, 256), preferred_element_type=F32)
        hidden = gate_act / (1.0 + jnp.exp(-gate_act)) * up_act
        hidden_ref[pl.ds(low, tile), :] = hidden.astype(BF16)
        return carry

    lax.fori_loop(0, rows.shape[0] // tile, first, 0)

    down_ref[...] = down_out[...].reshape(8, 256, 256)
    lowered(hidden_ref, down_ref, x, 1 - c, send_ref, (2,))


def expert(place, mine, theirs, slabs):
    count = mine.shape[1]
    matrix = jax.ShapeDtypeStruct((8, 8, 32, 256), BF16)
    return pl.pallas_call(
        expert_kernel,
        out_shape=(
            matrix,
            matrix,
            matrix,
            jax.ShapeDtypeStruct((8, 256, 256), BF16),
            jax.ShapeDtypeStruct((count, 256), BF16),
            jax.ShapeDtypeStruct((1, count, 256), BF16),
        ),
        in_specs=[SMEM] + [VMEM] * 10,
        out_specs=(VMEM,) * 6,
        scratch_shapes=[pltpu.VMEM((count, 2048), BF16)],
        compiler_params=pltpu.CompilerParams(vmem_limit_bytes=17 * 1024 * 1024),
        name="expert",
        cost_estimate=pl.CostEstimate(flops=8_000_000_000, bytes_accessed=12000000, transcendentals=0),
    )(place, mine, theirs, *slabs)


def far_kernel(place, hidden, down, own, send):
    lowered(hidden, down, place[0], place[1], own, (2,))
    lowered(hidden, down, place[0], 1 - place[1], send, (1, 3, 0))


def rest_kernel(place, hidden, down, own):
    lowered(hidden, down, place[0], place[1], own, (1, 3, 0))


def blocks(kernel, counts, place, hidden, down):
    shapes = [jax.ShapeDtypeStruct((n,) + hidden.shape, BF16) for n in counts]
    return pl.pallas_call(
        kernel,
        out_shape=shapes,
        in_specs=[SMEM, VMEM, VMEM],
        out_specs=[VMEM] * len(counts),
        compiler_params=pltpu.CompilerParams(vmem_limit_bytes=8 * 1024 * 1024),
        cost_estimate=pl.CostEstimate(flops=1_000_000_000, bytes_accessed=1500000, transcendentals=0),
    )(place, hidden, down)


def combine_kernel(plan_ref, back_ref, out_ref):
    rows, slots = plan_ref.shape[0], back_ref.shape[0]
    slot = lax.broadcasted_iota(jnp.int32, (rows, slots), 1)
    back = back_ref[...]
    picked = []
    for k in range(2):
        dest = (plan_ref[:, k : k + 1] + 0.5).astype(jnp.int32)
        onehot = jnp.where(slot == dest, 1.0, 0.0).astype(BF16)
        picked.append(jnp.dot(onehot, back, preferred_element_type=F32))
    out_ref[...] = (plan_ref[:, 2:3] * picked[0] + plan_ref[:, 3:4] * picked[1]).astype(BF16)


def combine(planned, back):
    return pl.pallas_call(
        combine_kernel,
        out_shape=jax.ShapeDtypeStruct((planned.shape[0], 256), BF16),
        in_specs=[VMEM, VMEM],
        out_specs=VMEM,
        compiler_params=pltpu.CompilerParams(vmem_limit_bytes=6 * 1024 * 1024),
        name="combine",
        cost_estimate=pl.CostEstimate(flops=1_000_000_000, bytes_accessed=600000, transcendentals=0),
    )(planned, back)


def assemble_kernel(ring_ref, out_ref):
    for x in range(4):
        for c in range(2):
            low = (c * 4 + x) * 256
            out_ref[:, low : low + 256] = ring_ref[2 * x + c]


def assemble(ring):
    rows = ring.shape[1]
    return pl.pallas_call(
        assemble_kernel,
        out_shape=jax.ShapeDtypeStruct((rows, 2048), BF16),
        in_specs=[VMEM],
        out_specs=VMEM,
        compiler_params=pltpu.CompilerParams(vmem_limit_bytes=6 * 1024 * 1024),
        name="assemble",
        cost_estimate=pl.CostEstimate(flops=100_000_000, bytes_accessed=1600000, transcendentals=0),
    )(ring)


def ring_of(value):
    pieces, first, second = [value], value, value
    for hop in range(1, 5):
        first = turn(first, "y", 1)
        pieces.append(first)
        if hop < 4:
            second = turn(second, "y", -1)
            pieces.append(second)
    return pieces


def layer(tokens, route_ids, route_logits, norm_gain, gate_weight, up_weight, down_weight):
    experts = gate_weight.shape[0]
    x, c = lax.axis_index("x"), lax.axis_index("c")
    place = jnp.stack([x, c, lax.axis_index("y")]).astype(jnp.int32)
    packed = fold(norm_gain, gate_weight, up_weight, down_weight)
    slab = lax.all_to_all(packed, "z", split_axis=0, concat_axis=0, tiled=True)
    slabs = ring_of(slab)

    sent = dispatch(place, route_ids.T, tokens, experts).reshape(experts, CAP, 256)
    arrived = lax.all_to_all(sent, "z", split_axis=0, concat_axis=0, tiled=True)
    arrived = arrived.reshape(1, -1, 256)
    spread = jnp.broadcast_to(arrived, (4,) + arrived.shape[1:])
    mine = lax.all_to_all(spread, "x", split_axis=0, concat_axis=0, tiled=True)
    theirs = swap(mine)

    gate_new, up_new, down_new, down, hidden, send = expert(place, mine, theirs, slabs)
    received = swap(send)
    own, send = blocks(far_kernel, (1, 3), place, hidden, down)
    far = turn((own[0].astype(F32) + received[0].astype(F32)).astype(BF16), "x", 1)
    received = swap(send)
    (own,) = blocks(rest_kernel, (3,), place, hidden, down)
    pairs = [own[j].astype(F32) + received[j].astype(F32) for j in range(3)]
    ahead = turn((pairs[0] + far.astype(F32)).astype(BF16), "x", 1)
    behind = turn(pairs[1].astype(BF16), "x", -1)
    share = (pairs[2] + behind.astype(F32) + ahead.astype(F32)).astype(BF16)
    back = lax.all_to_all(
        share.reshape(experts, CAP, 256), "z", split_axis=0, concat_axis=0, tiled=True
    ).reshape(-1, 256)
    mixed = combine(plan(route_ids, route_logits), back)
    ring = lax.all_gather(mixed, ("x", "c"), axis=0, tiled=False)
    mixed = assemble(ring)
    shape = (1, 2048, 256)
    return (mixed, gate_new.reshape(shape), up_new.reshape(shape), down_new.reshape(shape))


def solution(mesh):
    grid = Mesh(mesh.devices.reshape(8, 8, 4, 2), ("z", "y", "x", "c"))
    fs, tp = ("z", "y"), ("x", "c")
    return jax.shard_map(
        layer,
        mesh=grid,
        in_specs=(
            P(fs, None),
            P(fs, None),
            P(fs, None),
            P(fs),
            P(None, fs, tp),
            P(None, fs, tp),
            P(None, fs, tp),
        ),
        out_specs=(P(fs, None), P(fs, None, tp), P(fs, None, tp), P(fs, None, tp)),
        check_vma=False,
    )
```

```python
import functools

import jax
import jax.numpy as jnp
from jax import lax
from jax.experimental import pallas as pl
from jax.experimental.pallas import tpu as pltpu
from jax.sharding import Mesh
from jax.sharding import PartitionSpec as P


CAP = 96
BF16 = jnp.bfloat16
F32 = jnp.float32
VMEM = pl.BlockSpec(memory_space=pltpu.VMEM)
SMEM = pl.BlockSpec(memory_space=pltpu.SMEM)
HBM = pl.BlockSpec(memory_space=pltpu.HBM)


def turn(value, axis, by):
    size = lax.axis_size(axis)
    pairs = [(2 * i, 2 * ((i + by) % size)) for i in range(size)]
    pairs += [(2 * i + 1, 2 * ((i - by) % size) + 1) for i in range(size)]
    return lax.ppermute(value, (axis, "c"), pairs)


def swap(value):
    return lax.ppermute(value, "c", [(0, 1), (1, 0)])


def fold_kernel(gain_ref, gate_ref, up_ref, down_ref, out_ref, gain_buf, buffers, sems):
    copies = [pltpu.make_async_copy(gain_ref, gain_buf, sems.at[3])]
    for k, ref in enumerate((gate_ref, up_ref, down_ref)):
        copies.append(pltpu.make_async_copy(ref, buffers.at[k], sems.at[k]))
    for copy in copies:
        copy.start()
    for copy in copies[:2]:
        copy.wait()
    size = gain_ref.shape[1]
    row = lax.broadcasted_iota(jnp.int32, (size, size), 0)
    column = lax.broadcasted_iota(jnp.int32, (size, size), 1)
    gain = jnp.sum(jnp.where(row == column, gain_buf[...], 0.0), axis=1, keepdims=True)
    for e in range(out_ref.shape[0]):
        out_ref[e, 0] = (gain * buffers[0, e]).astype(BF16)
    copies[2].wait()
    for e in range(out_ref.shape[0]):
        out_ref[e, 1] = (gain * buffers[1, e]).astype(BF16)
    copies[3].wait()
    for e in range(out_ref.shape[0]):
        out_ref[e, 2] = buffers[2, e].astype(BF16)


def fold(gain, gate, up, down):
    experts, rows, columns = gate.shape
    return pl.pallas_call(
        fold_kernel,
        out_shape=jax.ShapeDtypeStruct((experts, 3, rows, columns), BF16),
        in_specs=[HBM] * 4,
        out_specs=VMEM,
        scratch_shapes=[
            pltpu.VMEM((1, rows), F32),
            pltpu.VMEM((3, experts, rows, columns), F32),
            pltpu.SemaphoreType.DMA((4,)),
        ],
        name="fold",
        cost_estimate=pl.CostEstimate(flops=500_000_000, bytes_accessed=1200000, transcendentals=0),
    )(gain.reshape(1, rows), gate, up, down)


def dispatch_kernel(experts, place, ids_ref, tokens_ref, out_ref):
    rows = tokens_ref.shape[0]
    values = tokens_ref[...].astype(F32)
    center = jnp.mean(values, axis=1, keepdims=True)
    spread = jnp.mean(jnp.square(values - center), axis=1, keepdims=True)
    width = out_ref.shape[1]
    start = pl.multiple_of(place[1] * width, width)
    own = tokens_ref[:, pl.ds(start, width)].astype(F32)
    normed = ((own - center) * lax.rsqrt(spread + 1e-06)).astype(BF16)
    first, second = ids_ref[0:1, :], ids_ref[1:2, :]
    expert = lax.broadcasted_iota(jnp.int32, (experts, rows), 0)
    chosen = jnp.where((expert == first) | (expert == second), 1.0, 0.0)
    earlier = jnp.where(
        lax.broadcasted_iota(jnp.int32, (rows, rows), 0)
        < lax.broadcasted_iota(jnp.int32, (rows, rows), 1),
        1.0,
        0.0,
    )
    rank = jnp.dot(chosen.astype(BF16), earlier.astype(BF16), preferred_element_type=F32)
    slots = (rank + 0.5).astype(jnp.int32) + expert * CAP
    dest0 = jnp.sum(jnp.where(expert == first, slots, 0), axis=0, keepdims=True)
    dest1 = jnp.sum(jnp.where(expert == second, slots, 0), axis=0, keepdims=True)
    slot = lax.broadcasted_iota(jnp.int32, (experts * CAP, rows), 0)
    picks = jnp.where((slot == dest0) | (slot == dest1), 1.0, 0.0).astype(BF16)
    out_ref[...] = jnp.dot(picks, normed, preferred_element_type=F32).astype(BF16)


def dispatch(place, ids, tokens, experts):
    return pl.pallas_call(
        functools.partial(dispatch_kernel, experts),
        out_shape=jax.ShapeDtypeStruct((experts * CAP, tokens.shape[1] // 2), BF16),
        in_specs=[SMEM, VMEM, VMEM],
        out_specs=VMEM,
        compiler_params=pltpu.CompilerParams(vmem_limit_bytes=16 * 1024 * 1024),
        name="dispatch",
        cost_estimate=pl.CostEstimate(flops=2_000_000_000, bytes_accessed=1200000, transcendentals=0),
    )(place, ids, tokens)


def plan_kernel(ids_ref, logits_ref, out_ref):
    rows = ids_ref.shape[0]
    first, second = ids_ref[:, 0:1], ids_ref[:, 1:2]
    expert = lax.broadcasted_iota(jnp.int32, (rows, 128), 1)
    chosen = jnp.where((expert == first) | (expert == second), 1.0, 0.0)
    earlier = jnp.where(
        lax.broadcasted_iota(jnp.int32, (rows, rows), 1)
        < lax.broadcasted_iota(jnp.int32, (rows, rows), 0),
        1.0,
        0.0,
    )
    rank = jnp.dot(earlier.astype(BF16), chosen.astype(BF16), preferred_element_type=F32)
    slots = rank + (expert * CAP).astype(F32)
    dest0 = jnp.sum(jnp.where(expert == first, slots, 0.0), axis=1, keepdims=True)
    dest1 = jnp.sum(jnp.where(expert == second, slots, 0.0), axis=1, keepdims=True)
    weight0 = jax.nn.sigmoid(logits_ref[:, 0:1] - logits_ref[:, 1:2])
    weight1 = jax.nn.sigmoid(logits_ref[:, 1:2] - logits_ref[:, 0:1])
    column = lax.broadcasted_iota(jnp.int32, (rows, 128), 1)
    out_ref[...] = jnp.where(
        column == 0,
        dest0,
        jnp.where(column == 1, dest1, jnp.where(column == 2, weight0, weight1)),
    )


def plan(ids, logits):
    return pl.pallas_call(
        plan_kernel,
        out_shape=jax.ShapeDtypeStruct((ids.shape[0], 128), F32),
        in_specs=[VMEM, VMEM],
        out_specs=VMEM,
        compiler_params=pltpu.CompilerParams(vmem_limit_bytes=4 * 1024 * 1024),
        name="plan",
        cost_estimate=pl.CostEstimate(flops=1_000_000_000, bytes_accessed=200000, transcendentals=0),
    )(ids, logits)


def lowered(hidden, down, x, side, out, which):
    ahead = 1 - 2 * side
    offsets = (0, ahead, 2, -ahead)
    for j, k in enumerate(which):
        part = down[pl.ds(side * 4 + lax.rem(x + 4 + offsets[k], 4), 1)].reshape(256, 256)
        out[j] = lax.dot_general(
            hidden[...], part, (((1,), (1,)), ((), ())), preferred_element_type=F32
        ).astype(BF16)


def expert_kernel(place, *refs):
    sides, slabs = refs[:2], refs[2:10]
    gate_out, up_out, down_out, down_ref, hidden_ref, send_ref, rows = refs[10:]
    x, c, y = place[0], place[1], place[2]
    ahead = 1 - 2 * c
    for slab, hops in zip(slabs, (0, -1, 1, -2, 2, -3, 3, -4)):
        at = lax.rem(y + 8 + hops * ahead, 8)
        for k, out in enumerate((gate_out, up_out, down_out)):
            out[:, pl.ds(at, 1)] = slab[:, k : k + 1]
    width = sides[0].shape[1]
    for core in range(2):
        side = c if core == 0 else 1 - c
        rows[:, pl.ds(pl.multiple_of(side * width, width), width)] = sides[core][...]
    gate_act = jnp.dot(rows[...], gate_out[...].reshape(2048, 256), preferred_element_type=F32)
    up_act = jnp.dot(rows[...], up_out[...].reshape(2048, 256), preferred_element_type=F32)
    hidden_ref[...] = (gate_act / (1.0 + jnp.exp(-gate_act)) * up_act).astype(BF16)
    down_ref[...] = down_out[...].reshape(8, 256, 256)
    lowered(hidden_ref, down_ref, x, 1 - c, send_ref, (2,))


def expert(place, mine, theirs, slabs):
    count = mine.shape[0]
    matrix = jax.ShapeDtypeStruct((8, 8, 32, 256), BF16)
    return pl.pallas_call(
        expert_kernel,
        out_shape=(
            matrix,
            matrix,
            matrix,
            jax.ShapeDtypeStruct((8, 256, 256), BF16),
            jax.ShapeDtypeStruct((count, 256), BF16),
            jax.ShapeDtypeStruct((1, count, 256), BF16),
        ),
        in_specs=[SMEM] + [VMEM] * 10,
        out_specs=(VMEM,) * 6,
        scratch_shapes=[pltpu.VMEM((count, 2048), BF16)],
        compiler_params=pltpu.CompilerParams(vmem_limit_bytes=17 * 1024 * 1024),
        name="expert",
        cost_estimate=pl.CostEstimate(flops=8_000_000_000, bytes_accessed=12000000, transcendentals=0),
    )(place, mine, theirs, *slabs)


def far_kernel(place, hidden, down, own, send):
    lowered(hidden, down, place[0], place[1], own, (2,))
    lowered(hidden, down, place[0], 1 - place[1], send, (1, 3, 0))


def rest_kernel(place, hidden, down, own):
    lowered(hidden, down, place[0], place[1], own, (1, 3, 0))


def blocks(kernel, counts, place, hidden, down):
    shapes = [jax.ShapeDtypeStruct((n,) + hidden.shape, BF16) for n in counts]
    return pl.pallas_call(
        kernel,
        out_shape=shapes,
        in_specs=[SMEM, VMEM, VMEM],
        out_specs=[VMEM] * len(counts),
        compiler_params=pltpu.CompilerParams(vmem_limit_bytes=8 * 1024 * 1024),
        cost_estimate=pl.CostEstimate(flops=1_000_000_000, bytes_accessed=1500000, transcendentals=0),
    )(place, hidden, down)


def combine_kernel(plan_ref, back_ref, out_ref):
    rows, slots = plan_ref.shape[0], back_ref.shape[0]
    slot = lax.broadcasted_iota(jnp.int32, (rows, slots), 1)
    back = back_ref[...]
    picked = []
    for k in range(2):
        dest = (plan_ref[:, k : k + 1] + 0.5).astype(jnp.int32)
        onehot = jnp.where(slot == dest, 1.0, 0.0).astype(BF16)
        picked.append(jnp.dot(onehot, back, preferred_element_type=F32))
    out_ref[...] = (plan_ref[:, 2:3] * picked[0] + plan_ref[:, 3:4] * picked[1]).astype(BF16)


def combine(planned, back):
    return pl.pallas_call(
        combine_kernel,
        out_shape=jax.ShapeDtypeStruct((planned.shape[0], 256), BF16),
        in_specs=[VMEM, VMEM],
        out_specs=VMEM,
        compiler_params=pltpu.CompilerParams(vmem_limit_bytes=6 * 1024 * 1024),
        name="combine",
        cost_estimate=pl.CostEstimate(flops=1_000_000_000, bytes_accessed=600000, transcendentals=0),
    )(planned, back)


def assemble_kernel(ring_ref, out_ref):
    for x in range(4):
        for c in range(2):
            low = (c * 4 + x) * 256
            out_ref[:, low : low + 256] = ring_ref[2 * x + c]


def assemble(ring):
    rows = ring.shape[1]
    return pl.pallas_call(
        assemble_kernel,
        out_shape=jax.ShapeDtypeStruct((rows, 2048), BF16),
        in_specs=[VMEM],
        out_specs=VMEM,
        compiler_params=pltpu.CompilerParams(vmem_limit_bytes=6 * 1024 * 1024),
        name="assemble",
        cost_estimate=pl.CostEstimate(flops=100_000_000, bytes_accessed=1600000, transcendentals=0),
    )(ring)


def ring_of(value):
    pieces, first, second = [value], value, value
    for hop in range(1, 5):
        first = turn(first, "y", 1)
        pieces.append(first)
        if hop < 4:
            second = turn(second, "y", -1)
            pieces.append(second)
    return pieces


def layer(tokens, route_ids, route_logits, norm_gain, gate_weight, up_weight, down_weight):
    experts = gate_weight.shape[0]
    x, c = lax.axis_index("x"), lax.axis_index("c")
    place = jnp.stack([x, c, lax.axis_index("y")]).astype(jnp.int32)
    packed = fold(norm_gain, gate_weight, up_weight, down_weight)
    slab = lax.all_to_all(packed, "z", split_axis=0, concat_axis=0, tiled=True)
    slabs = ring_of(slab)

    sent = dispatch(place, route_ids.T, tokens, experts).reshape(experts, CAP, -1)
    arrived = lax.all_to_all(sent, "z", split_axis=0, concat_axis=0, tiled=True)
    mine = arrived.reshape(-1, arrived.shape[2])
    theirs = swap(mine)

    gate_new, up_new, down_new, down, hidden, send = expert(place, mine, theirs, slabs)
    received = swap(send)
    own, send = blocks(far_kernel, (1, 3), place, hidden, down)
    far = turn((own[0].astype(F32) + received[0].astype(F32)).astype(BF16), "x", 1)
    received = swap(send)
    (own,) = blocks(rest_kernel, (3,), place, hidden, down)
    pairs = [own[j].astype(F32) + received[j].astype(F32) for j in range(3)]
    ahead = turn((pairs[0] + far.astype(F32)).astype(BF16), "x", 1)
    behind = turn(pairs[1].astype(BF16), "x", -1)
    share = (pairs[2] + behind.astype(F32) + ahead.astype(F32)).astype(BF16)
    back = lax.all_to_all(
        share.reshape(experts, CAP, 256), "z", split_axis=0, concat_axis=0, tiled=True
    ).reshape(-1, 256)
    mixed = combine(plan(route_ids, route_logits), back)
    ring = lax.all_gather(mixed, ("x", "c"), axis=0, tiled=False)
    mixed = assemble(ring)
    shape = (1, 2048, 256)
    return (mixed, gate_new.reshape(shape), up_new.reshape(shape), down_new.reshape(shape))


def solution(mesh):
    grid = Mesh(mesh.devices.reshape(8, 8, 4, 2), ("z", "y", "x", "c"))
    fs, tp = ("z", "y"), ("x", "c")
    return jax.shard_map(
        layer,
        mesh=grid,
        in_specs=(
            P(fs, None),
            P(fs, None),
            P(fs, None),
            P(fs),
            P(None, fs, tp),
            P(None, fs, tp),
            P(None, fs, tp),
        ),
        out_specs=(P(fs, None), P(fs, None, tp), P(fs, None, tp), P(fs, None, tp)),
        check_vma=False,
    )
```

```python
import functools

import jax
import jax.numpy as jnp
from jax import lax
from jax.experimental import pallas as pl
from jax.experimental.pallas import tpu as pltpu
from jax.sharding import Mesh
from jax.sharding import PartitionSpec as P


CAP = 96
CUT = 2
BF16 = jnp.bfloat16
F32 = jnp.float32
VMEM = pl.BlockSpec(memory_space=pltpu.VMEM)
SMEM = pl.BlockSpec(memory_space=pltpu.SMEM)
HBM = pl.BlockSpec(memory_space=pltpu.HBM)


def meet(value, axis, late):
    size = lax.axis_size(axis)
    pairs = []
    for i in range(size):
        for core in range(2):
            step = (1 - 2 * ((i + core) % 2)) * (-1 if late else 1)
            pairs.append((2 * i + core, 2 * ((i + step) % size) + core))
    return lax.ppermute(value, (axis, "c"), pairs)


def swap(value):
    return lax.ppermute(value, "c", [(0, 1), (1, 0)])


def fold_kernel(gain_ref, gate_ref, up_ref, down_ref, out_ref, gain_buf, buffers, sems):
    copies = [pltpu.make_async_copy(gain_ref, gain_buf, sems.at[3])]
    for k, ref in enumerate((gate_ref, up_ref, down_ref)):
        copies.append(pltpu.make_async_copy(ref, buffers.at[k], sems.at[k]))
    for copy in copies:
        copy.start()
    for copy in copies[:2]:
        copy.wait()
    size = gain_ref.shape[1]
    row = lax.broadcasted_iota(jnp.int32, (size, size), 0)
    column = lax.broadcasted_iota(jnp.int32, (size, size), 1)
    gain = jnp.sum(jnp.where(row == column, gain_buf[...], 0.0), axis=1, keepdims=True)
    for e in range(out_ref.shape[0]):
        out_ref[e, 0] = (gain * buffers[0, e]).astype(BF16)
    copies[2].wait()
    for e in range(out_ref.shape[0]):
        out_ref[e, 1] = (gain * buffers[1, e]).astype(BF16)
    copies[3].wait()
    for e in range(out_ref.shape[0]):
        out_ref[e, 2] = buffers[2, e].astype(BF16)


def fold(gain, gate, up, down):
    experts, rows, columns = gate.shape
    return pl.pallas_call(
        fold_kernel,
        out_shape=jax.ShapeDtypeStruct((experts, 3, rows, columns), BF16),
        in_specs=[HBM] * 4,
        out_specs=VMEM,
        scratch_shapes=[
            pltpu.VMEM((1, rows), F32),
            pltpu.VMEM((3, experts, rows, columns), F32),
            pltpu.SemaphoreType.DMA((4,)),
        ],
        name="fold",
        cost_estimate=pl.CostEstimate(flops=500_000_000, bytes_accessed=1200000, transcendentals=0),
    )(gain.reshape(1, rows), gate, up, down)


def dispatch_kernel(experts, place, ids_ref, tokens_ref, out_ref):
    rows = tokens_ref.shape[0]
    values = tokens_ref[...].astype(F32)
    center = jnp.mean(values, axis=1, keepdims=True)
    spread = jnp.mean(jnp.square(values - center), axis=1, keepdims=True)
    width = out_ref.shape[1]
    start = pl.multiple_of(place[1] * width, width)
    own = tokens_ref[:, pl.ds(start, width)].astype(F32)
    normed = ((own - center) * lax.rsqrt(spread + 1e-06)).astype(BF16)
    first, second = ids_ref[0:1, :], ids_ref[1:2, :]
    expert = lax.broadcasted_iota(jnp.int32, (experts, rows), 0)
    chosen = jnp.where((expert == first) | (expert == second), 1.0, 0.0)
    earlier = jnp.where(
        lax.broadcasted_iota(jnp.int32, (rows, rows), 0)
        < lax.broadcasted_iota(jnp.int32, (rows, rows), 1),
        1.0,
        0.0,
    )
    rank = jnp.dot(chosen.astype(BF16), earlier.astype(BF16), preferred_element_type=F32)
    slots = (rank + 0.5).astype(jnp.int32) + expert * CAP
    dest0 = jnp.sum(jnp.where(expert == first, slots, 0), axis=0, keepdims=True)
    dest1 = jnp.sum(jnp.where(expert == second, slots, 0), axis=0, keepdims=True)
    slot = lax.broadcasted_iota(jnp.int32, (experts * CAP, rows), 0)
    picks = jnp.where((slot == dest0) | (slot == dest1), 1.0, 0.0).astype(BF16)
    out_ref[...] = jnp.dot(picks, normed, preferred_element_type=F32).astype(BF16)


def dispatch(place, ids, tokens, experts):
    return pl.pallas_call(
        functools.partial(dispatch_kernel, experts),
        out_shape=jax.ShapeDtypeStruct((experts * CAP, tokens.shape[1] // 2), BF16),
        in_specs=[SMEM, VMEM, VMEM],
        out_specs=VMEM,
        compiler_params=pltpu.CompilerParams(vmem_limit_bytes=16 * 1024 * 1024),
        name="dispatch",
        cost_estimate=pl.CostEstimate(flops=2_000_000_000, bytes_accessed=1200000, transcendentals=0),
    )(place, ids, tokens)


def plan_kernel(ids_ref, logits_ref, out_ref):
    rows = ids_ref.shape[0]
    first, second = ids_ref[:, 0:1], ids_ref[:, 1:2]
    expert = lax.broadcasted_iota(jnp.int32, (rows, 128), 1)
    chosen = jnp.where((expert == first) | (expert == second), 1.0, 0.0)
    earlier = jnp.where(
        lax.broadcasted_iota(jnp.int32, (rows, rows), 1)
        < lax.broadcasted_iota(jnp.int32, (rows, rows), 0),
        1.0,
        0.0,
    )
    rank = jnp.dot(earlier.astype(BF16), chosen.astype(BF16), preferred_element_type=F32)
    slots = rank + (expert * CAP).astype(F32)
    dest0 = jnp.sum(jnp.where(expert == first, slots, 0.0), axis=1, keepdims=True)
    dest1 = jnp.sum(jnp.where(expert == second, slots, 0.0), axis=1, keepdims=True)
    weight0 = jax.nn.sigmoid(logits_ref[:, 0:1] - logits_ref[:, 1:2])
    weight1 = jax.nn.sigmoid(logits_ref[:, 1:2] - logits_ref[:, 0:1])
    column = lax.broadcasted_iota(jnp.int32, (rows, 128), 1)
    out_ref[...] = jnp.where(
        column == 0,
        dest0,
        jnp.where(column == 1, dest1, jnp.where(column == 2, weight0, weight1)),
    )


def plan(ids, logits):
    return pl.pallas_call(
        plan_kernel,
        out_shape=jax.ShapeDtypeStruct((ids.shape[0], 128), F32),
        in_specs=[VMEM, VMEM],
        out_specs=VMEM,
        compiler_params=pltpu.CompilerParams(vmem_limit_bytes=4 * 1024 * 1024),
        name="plan",
        cost_estimate=pl.CostEstimate(flops=1_000_000_000, bytes_accessed=200000, transcendentals=0),
    )(ids, logits)


def lowered(hidden, down, x, side, out, which):
    ahead = 1 - 2 * lax.rem(x + side, 2)
    offsets = (0, ahead, 2, -ahead)
    for j, k in enumerate(which):
        part = down[pl.ds(side * 4 + lax.rem(x + 4 + offsets[k], 4), 1)].reshape(256, 256)
        out[j] = lax.dot_general(
            hidden[...], part, (((1,), (1,)), ((), ())), preferred_element_type=F32
        ).astype(BF16)


def expert_kernel(place, *refs):
    sides, slabs = refs[:2], refs[2 : 3 + 4 * CUT]
    gate_out, up_out, down_out, down_ref, hidden_ref, send_ref, rows = refs[3 + 4 * CUT :]
    x, c, y = place[0], place[1], place[2]
    step = 1 - 2 * lax.rem(y + c, 2)
    size = 8 // CUT
    for k, out in enumerate((gate_out, up_out, down_out)):
        out[:, pl.ds(y, 1)] = slabs[0][:, k : k + 1]
        for n in range(CUT):
            low = n * size
            for hop, offsets in enumerate(((1,), (-1, -2), (2, 3), (-3, -4))):
                slab = slabs[1 + hop * CUT + n]
                for m, offset in enumerate(offsets):
                    at = lax.rem(y + 8 + offset * step, 8)
                    piece = slab[:, k : k + 1] if hop == 0 else slab[m, :, k : k + 1]
                    out[low : low + size, pl.ds(at, 1)] = piece
    width = sides[0].shape[1]
    for core in range(2):
        side = c if core == 0 else 1 - c
        rows[:, pl.ds(pl.multiple_of(side * width, width), width)] = sides[core][...]
    gate_act = jnp.dot(rows[...], gate_out[...].reshape(2048, 256), preferred_element_type=F32)
    up_act = jnp.dot(rows[...], up_out[...].reshape(2048, 256), preferred_element_type=F32)
    hidden_ref[...] = (gate_act / (1.0 + jnp.exp(-gate_act)) * up_act).astype(BF16)
    down_ref[...] = down_out[...].reshape(8, 256, 256)
    lowered(hidden_ref, down_ref, x, 1 - c, send_ref, (3, 2))


def expert(place, mine, theirs, slabs):
    count = mine.shape[0]
    matrix = jax.ShapeDtypeStruct((8, 8, 32, 256), BF16)
    return pl.pallas_call(
        expert_kernel,
        out_shape=(
            matrix,
            matrix,
            matrix,
            jax.ShapeDtypeStruct((8, 256, 256), BF16),
            jax.ShapeDtypeStruct((count, 256), BF16),
            jax.ShapeDtypeStruct((2, count, 256), BF16),
        ),
        in_specs=[SMEM] + [VMEM] * (3 + 4 * CUT),
        out_specs=(VMEM,) * 6,
        scratch_shapes=[pltpu.VMEM((count, 2048), BF16)],
        compiler_params=pltpu.CompilerParams(vmem_limit_bytes=17 * 1024 * 1024),
        name="expert",
        cost_estimate=pl.CostEstimate(flops=8_000_000_000, bytes_accessed=12000000, transcendentals=0),
    )(place, mine, theirs, *slabs)


def far_kernel(place, hidden, down, own, send):
    lowered(hidden, down, place[0], place[1], own, (3, 2))
    lowered(hidden, down, place[0], 1 - place[1], send, (1, 0))


def rest_kernel(place, hidden, down, own):
    lowered(hidden, down, place[0], place[1], own, (1, 0))


def blocks(kernel, counts, place, hidden, down):
    shapes = [jax.ShapeDtypeStruct((n,) + hidden.shape, BF16) for n in counts]
    return pl.pallas_call(
        kernel,
        out_shape=shapes,
        in_specs=[SMEM, VMEM, VMEM],
        out_specs=[VMEM] * len(counts),
        compiler_params=pltpu.CompilerParams(vmem_limit_bytes=8 * 1024 * 1024),
        cost_estimate=pl.CostEstimate(flops=1_000_000_000, bytes_accessed=1500000, transcendentals=0),
    )(place, hidden, down)


def combine_kernel(plan_ref, back_ref, out_ref):
    rows, slots = plan_ref.shape[0], back_ref.shape[0]
    slot = lax.broadcasted_iota(jnp.int32, (rows, slots), 1)
    back = back_ref[...]
    picked = []
    for k in range(2):
        dest = (plan_ref[:, k : k + 1] + 0.5).astype(jnp.int32)
        onehot = jnp.where(slot == dest, 1.0, 0.0).astype(BF16)
        picked.append(jnp.dot(onehot, back, preferred_element_type=F32))
    out_ref[...] = (plan_ref[:, 2:3] * picked[0] + plan_ref[:, 3:4] * picked[1]).astype(BF16)


def combine(planned, back):
    return pl.pallas_call(
        combine_kernel,
        out_shape=jax.ShapeDtypeStruct((planned.shape[0], 256), BF16),
        in_specs=[VMEM, VMEM],
        out_specs=VMEM,
        compiler_params=pltpu.CompilerParams(vmem_limit_bytes=6 * 1024 * 1024),
        name="combine",
        cost_estimate=pl.CostEstimate(flops=1_000_000_000, bytes_accessed=600000, transcendentals=0),
    )(planned, back)


def assemble_kernel(ring_ref, out_ref):
    for x in range(4):
        for c in range(2):
            low = (c * 4 + x) * 256
            out_ref[:, low : low + 256] = ring_ref[2 * x + c]


def assemble(ring):
    rows = ring.shape[1]
    return pl.pallas_call(
        assemble_kernel,
        out_shape=jax.ShapeDtypeStruct((rows, 2048), BF16),
        in_specs=[VMEM],
        out_specs=VMEM,
        compiler_params=pltpu.CompilerParams(vmem_limit_bytes=6 * 1024 * 1024),
        name="assemble",
        cost_estimate=pl.CostEstimate(flops=100_000_000, bytes_accessed=1600000, transcendentals=0),
    )(ring)


def gathered(value):
    parts = value.shape[0] // CUT
    pieces, held = [value], [value[n * parts : (n + 1) * parts] for n in range(CUT)]
    for hop in range(1, 5):
        for n in range(CUT):
            piece = meet(held[n], "y", hop % 2 == 0)
            held[n] = jnp.stack([held[n], piece]) if hop == 1 else piece
            pieces.append(piece)
    return pieces


def layer(tokens, route_ids, route_logits, norm_gain, gate_weight, up_weight, down_weight):
    experts = gate_weight.shape[0]
    x, c = lax.axis_index("x"), lax.axis_index("c")
    place = jnp.stack([x, c, lax.axis_index("y")]).astype(jnp.int32)
    packed = fold(norm_gain, gate_weight, up_weight, down_weight)
    slab = lax.all_to_all(packed, "z", split_axis=0, concat_axis=0, tiled=True)
    slabs = gathered(slab)

    sent = dispatch(place, route_ids.T, tokens, experts).reshape(experts, CAP, -1)
    arrived = lax.all_to_all(sent, "z", split_axis=0, concat_axis=0, tiled=True)
    mine = arrived.reshape(-1, arrived.shape[2])
    theirs = swap(mine)

    gate_new, up_new, down_new, down, hidden, send = expert(place, mine, theirs, slabs)
    received = swap(send)
    own, send = blocks(far_kernel, (2, 2), place, hidden, down)
    came = meet((own.astype(F32) + received.astype(F32)).astype(BF16), "x", True)
    received = swap(send)
    (own,) = blocks(rest_kernel, (2,), place, hidden, down)
    onward = own[0].astype(F32) + received[0].astype(F32) + came[1].astype(F32)
    last = meet(onward.astype(BF16), "x", False)
    share = own[1].astype(F32) + received[1].astype(F32) + came[0].astype(F32)
    share = (share + last.astype(F32)).astype(BF16)
    back = lax.all_to_all(
        share.reshape(experts, CAP, 256), "z", split_axis=0, concat_axis=0, tiled=True
    ).reshape(-1, 256)
    mixed = combine(plan(route_ids, route_logits), back)
    ring = lax.all_gather(mixed, ("x", "c"), axis=0, tiled=False)
    mixed = assemble(ring)
    shape = (1, 2048, 256)
    return (mixed, gate_new.reshape(shape), up_new.reshape(shape), down_new.reshape(shape))


def solution(mesh):
    grid = Mesh(mesh.devices.reshape(8, 8, 4, 2), ("z", "y", "x", "c"))
    fs, tp = ("z", "y"), ("x", "c")
    return jax.shard_map(
        layer,
        mesh=grid,
        in_specs=(
            P(fs, None),
            P(fs, None),
            P(fs, None),
            P(fs),
            P(None, fs, tp),
            P(None, fs, tp),
            P(None, fs, tp),
        ),
        out_specs=(P(fs, None), P(fs, None, tp), P(fs, None, tp), P(fs, None, tp)),
        check_vma=False,
    )
```

```python
import functools

import jax
import jax.numpy as jnp
from jax import lax
from jax.experimental import pallas as pl
from jax.experimental.pallas import tpu as pltpu
from jax.sharding import Mesh
from jax.sharding import PartitionSpec as P


CAP = 96
CUT = 2
BF16 = jnp.bfloat16
F32 = jnp.float32
VMEM = pl.BlockSpec(memory_space=pltpu.VMEM)
SMEM = pl.BlockSpec(memory_space=pltpu.SMEM)
HBM = pl.BlockSpec(memory_space=pltpu.HBM)


def meet(value, axis, late):
    size = lax.axis_size(axis)
    pairs = []
    for i in range(size):
        for core in range(2):
            step = (1 - 2 * ((i + core) % 2)) * (-1 if late else 1)
            pairs.append((2 * i + core, 2 * ((i + step) % size) + core))
    return lax.ppermute(value, (axis, "c"), pairs)


def swap(value):
    return lax.ppermute(value, "c", [(0, 1), (1, 0)])


def fold_kernel(gain_ref, gate_ref, up_ref, down_ref, out_ref, gain_buf, buffers, sems):
    copies = [pltpu.make_async_copy(gain_ref, gain_buf, sems.at[3])]
    for k, ref in enumerate((gate_ref, up_ref, down_ref)):
        copies.append(pltpu.make_async_copy(ref, buffers.at[k], sems.at[k]))
    for copy in copies:
        copy.start()
    for copy in copies[:2]:
        copy.wait()
    size = gain_ref.shape[1]
    row = lax.broadcasted_iota(jnp.int32, (size, size), 0)
    column = lax.broadcasted_iota(jnp.int32, (size, size), 1)
    gain = jnp.sum(jnp.where(row == column, gain_buf[...], 0.0), axis=1, keepdims=True)
    for e in range(out_ref.shape[0]):
        out_ref[e, 0] = (gain * buffers[0, e]).astype(BF16)
    copies[2].wait()
    for e in range(out_ref.shape[0]):
        out_ref[e, 1] = (gain * buffers[1, e]).astype(BF16)
    copies[3].wait()
    for e in range(out_ref.shape[0]):
        out_ref[e, 2] = buffers[2, e].astype(BF16)


def fold(gain, gate, up, down):
    experts, rows, columns = gate.shape
    return pl.pallas_call(
        fold_kernel,
        out_shape=jax.ShapeDtypeStruct((experts, 3, rows, columns), BF16),
        in_specs=[HBM] * 4,
        out_specs=VMEM,
        scratch_shapes=[
            pltpu.VMEM((1, rows), F32),
            pltpu.VMEM((3, experts, rows, columns), F32),
            pltpu.SemaphoreType.DMA((4,)),
        ],
        name="fold",
        cost_estimate=pl.CostEstimate(flops=500_000_000, bytes_accessed=1200000, transcendentals=0),
    )(gain.reshape(1, rows), gate, up, down)


def dispatch_kernel(experts, place, ids_ref, tokens_ref, out_ref):
    rows = tokens_ref.shape[0]
    values = tokens_ref[...].astype(F32)
    center = jnp.mean(values, axis=1, keepdims=True)
    spread = jnp.mean(jnp.square(values - center), axis=1, keepdims=True)
    width = out_ref.shape[1]
    start = pl.multiple_of(place[1] * width, width)
    own = tokens_ref[:, pl.ds(start, width)].astype(F32)
    normed = ((own - center) * lax.rsqrt(spread + 1e-06)).astype(BF16)
    first, second = ids_ref[0:1, :], ids_ref[1:2, :]
    expert = lax.broadcasted_iota(jnp.int32, (experts, rows), 0)
    chosen = jnp.where((expert == first) | (expert == second), 1.0, 0.0)
    earlier = jnp.where(
        lax.broadcasted_iota(jnp.int32, (rows, rows), 0)
        < lax.broadcasted_iota(jnp.int32, (rows, rows), 1),
        1.0,
        0.0,
    )
    rank = jnp.dot(chosen.astype(BF16), earlier.astype(BF16), preferred_element_type=F32)
    slots = (rank + 0.5).astype(jnp.int32) + expert * CAP
    dest0 = jnp.sum(jnp.where(expert == first, slots, 0), axis=0, keepdims=True)
    dest1 = jnp.sum(jnp.where(expert == second, slots, 0), axis=0, keepdims=True)
    slot = lax.broadcasted_iota(jnp.int32, (experts * CAP, rows), 0)
    picks = jnp.where((slot == dest0) | (slot == dest1), 1.0, 0.0).astype(BF16)
    out_ref[...] = jnp.dot(picks, normed, preferred_element_type=F32).astype(BF16)


def dispatch(place, ids, tokens, experts):
    return pl.pallas_call(
        functools.partial(dispatch_kernel, experts),
        out_shape=jax.ShapeDtypeStruct((experts * CAP, tokens.shape[1] // 2), BF16),
        in_specs=[SMEM, VMEM, VMEM],
        out_specs=VMEM,
        compiler_params=pltpu.CompilerParams(vmem_limit_bytes=16 * 1024 * 1024),
        name="dispatch",
        cost_estimate=pl.CostEstimate(flops=2_000_000_000, bytes_accessed=1200000, transcendentals=0),
    )(place, ids, tokens)


def plan_kernel(ids_ref, logits_ref, out_ref):
    rows = ids_ref.shape[0]
    first, second = ids_ref[:, 0:1], ids_ref[:, 1:2]
    expert = lax.broadcasted_iota(jnp.int32, (rows, 128), 1)
    chosen = jnp.where((expert == first) | (expert == second), 1.0, 0.0)
    earlier = jnp.where(
        lax.broadcasted_iota(jnp.int32, (rows, rows), 1)
        < lax.broadcasted_iota(jnp.int32, (rows, rows), 0),
        1.0,
        0.0,
    )
    rank = jnp.dot(earlier.astype(BF16), chosen.astype(BF16), preferred_element_type=F32)
    slots = rank + (expert * CAP).astype(F32)
    dest0 = jnp.sum(jnp.where(expert == first, slots, 0.0), axis=1, keepdims=True)
    dest1 = jnp.sum(jnp.where(expert == second, slots, 0.0), axis=1, keepdims=True)
    weight0 = jax.nn.sigmoid(logits_ref[:, 0:1] - logits_ref[:, 1:2])
    weight1 = jax.nn.sigmoid(logits_ref[:, 1:2] - logits_ref[:, 0:1])
    column = lax.broadcasted_iota(jnp.int32, (rows, 128), 1)
    out_ref[...] = jnp.where(
        column == 0,
        dest0,
        jnp.where(column == 1, dest1, jnp.where(column == 2, weight0, weight1)),
    )


def plan(ids, logits):
    return pl.pallas_call(
        plan_kernel,
        out_shape=jax.ShapeDtypeStruct((ids.shape[0], 128), F32),
        in_specs=[VMEM, VMEM],
        out_specs=VMEM,
        compiler_params=pltpu.CompilerParams(vmem_limit_bytes=4 * 1024 * 1024),
        name="plan",
        cost_estimate=pl.CostEstimate(flops=1_000_000_000, bytes_accessed=200000, transcendentals=0),
    )(ids, logits)


def lowered(hidden, down, x, side, out, which):
    ahead = 1 - 2 * lax.rem(x + side, 2)
    offsets = (0, ahead, 2, -ahead)
    for j, k in enumerate(which):
        part = down[pl.ds(side * 4 + lax.rem(x + 4 + offsets[k], 4), 1)].reshape(256, 256)
        out[j] = lax.dot_general(
            hidden[...], part, (((1,), (1,)), ((), ())), preferred_element_type=F32
        ).astype(BF16)


def expert_kernel(place, *refs):
    sides, slabs = refs[:2], refs[2 : 3 + 4 * CUT]
    gate_out, up_out, down_out, down_ref, hidden_ref, send_ref, rows = refs[3 + 4 * CUT :]
    x, c, y = place[0], place[1], place[2]
    step = 1 - 2 * lax.rem(y + c, 2)
    size = 8 // CUT
    for k, out in enumerate((gate_out, up_out, down_out)):
        out[:, pl.ds(y, 1)] = slabs[0][:, k : k + 1]
        for n in range(CUT):
            low = n * size
            for hop, offsets in enumerate(((1,), (-1, -2), (2, 3), (-3, -4))):
                slab = slabs[1 + hop * CUT + n]
                for m, offset in enumerate(offsets):
                    at = lax.rem(y + 8 + offset * step, 8)
                    piece = slab[:, k : k + 1] if hop == 0 else slab[m, :, k : k + 1]
                    out[low : low + size, pl.ds(at, 1)] = piece
    width = sides[0].shape[1]
    for core in range(2):
        side = c if core == 0 else 1 - c
        rows[:, pl.ds(pl.multiple_of(side * width, width), width)] = sides[core][...]
    gate_act = jnp.dot(rows[...], gate_out[...].reshape(2048, 256), preferred_element_type=F32)
    up_act = jnp.dot(rows[...], up_out[...].reshape(2048, 256), preferred_element_type=F32)
    hidden_ref[...] = (gate_act / (1.0 + jnp.exp(-gate_act)) * up_act).astype(BF16)
    down_ref[...] = down_out[...].reshape(8, 256, 256)
    lowered(hidden_ref, down_ref, x, 1 - c, send_ref, (3, 2))


def expert(place, mine, theirs, slabs):
    count = mine.shape[0]
    matrix = jax.ShapeDtypeStruct((8, 8, 32, 256), BF16)
    return pl.pallas_call(
        expert_kernel,
        out_shape=(
            matrix,
            matrix,
            matrix,
            jax.ShapeDtypeStruct((8, 256, 256), BF16),
            jax.ShapeDtypeStruct((count, 256), BF16),
            jax.ShapeDtypeStruct((2, count, 256), BF16),
        ),
        in_specs=[SMEM] + [VMEM] * (3 + 4 * CUT),
        out_specs=(VMEM,) * 6,
        scratch_shapes=[pltpu.VMEM((count, 2048), BF16)],
        compiler_params=pltpu.CompilerParams(vmem_limit_bytes=17 * 1024 * 1024),
        name="expert",
        cost_estimate=pl.CostEstimate(flops=8_000_000_000, bytes_accessed=12000000, transcendentals=0),
    )(place, mine, theirs, *slabs)


def far_kernel(place, hidden, down, own, send):
    lowered(hidden, down, place[0], place[1], own, (3, 2))
    lowered(hidden, down, place[0], 1 - place[1], send, (1, 0))


def rest_kernel(place, hidden, down, own):
    lowered(hidden, down, place[0], place[1], own, (1, 0))


def blocks(kernel, counts, place, hidden, down):
    shapes = [jax.ShapeDtypeStruct((n,) + hidden.shape, BF16) for n in counts]
    return pl.pallas_call(
        kernel,
        out_shape=shapes,
        in_specs=[SMEM, VMEM, VMEM],
        out_specs=[VMEM] * len(counts),
        compiler_params=pltpu.CompilerParams(vmem_limit_bytes=8 * 1024 * 1024),
        cost_estimate=pl.CostEstimate(flops=1_000_000_000, bytes_accessed=1500000, transcendentals=0),
    )(place, hidden, down)


def onward_kernel(low, own, received, came, out):
    rows = pl.ds(low, out.shape[0])
    total = own[0, rows].astype(F32) + received[0, rows].astype(F32) + came[1].astype(F32)
    out[...] = total.astype(BF16)


def finish_kernel(own, received, *refs):
    came, last, out = refs[:CUT], refs[CUT : 2 * CUT], refs[2 * CUT]
    size = out.shape[0] // CUT
    for n in range(CUT):
        rows = pl.ds(n * size, size)
        total = own[1, rows].astype(F32) + received[1, rows].astype(F32)
        total = total + came[n][0].astype(F32) + last[n][...].astype(F32)
        out[rows] = total.astype(BF16)


def added(kernel, rows, *args):
    return pl.pallas_call(
        kernel,
        out_shape=jax.ShapeDtypeStruct((rows, 256), BF16),
        in_specs=[VMEM] * len(args),
        out_specs=VMEM,
        compiler_params=pltpu.CompilerParams(vmem_limit_bytes=8 * 1024 * 1024),
        cost_estimate=pl.CostEstimate(flops=100_000_000, bytes_accessed=1500000, transcendentals=0),
    )(*args)


def combine_kernel(plan_ref, back_ref, out_ref):
    rows, slots = plan_ref.shape[0], back_ref.shape[0]
    slot = lax.broadcasted_iota(jnp.int32, (rows, slots), 1)
    back = back_ref[...]
    picked = []
    for k in range(2):
        dest = (plan_ref[:, k : k + 1] + 0.5).astype(jnp.int32)
        onehot = jnp.where(slot == dest, 1.0, 0.0).astype(BF16)
        picked.append(jnp.dot(onehot, back, preferred_element_type=F32))
    out_ref[...] = (plan_ref[:, 2:3] * picked[0] + plan_ref[:, 3:4] * picked[1]).astype(BF16)


def combine(planned, back):
    return pl.pallas_call(
        combine_kernel,
        out_shape=jax.ShapeDtypeStruct((planned.shape[0], 256), BF16),
        in_specs=[VMEM, VMEM],
        out_specs=VMEM,
        compiler_params=pltpu.CompilerParams(vmem_limit_bytes=6 * 1024 * 1024),
        name="combine",
        cost_estimate=pl.CostEstimate(flops=1_000_000_000, bytes_accessed=600000, transcendentals=0),
    )(planned, back)


def assemble_kernel(ring_ref, out_ref):
    for x in range(4):
        for c in range(2):
            low = (c * 4 + x) * 256
            out_ref[:, low : low + 256] = ring_ref[2 * x + c]


def assemble(ring):
    rows = ring.shape[1]
    return pl.pallas_call(
        assemble_kernel,
        out_shape=jax.ShapeDtypeStruct((rows, 2048), BF16),
        in_specs=[VMEM],
        out_specs=VMEM,
        compiler_params=pltpu.CompilerParams(vmem_limit_bytes=6 * 1024 * 1024),
        name="assemble",
        cost_estimate=pl.CostEstimate(flops=100_000_000, bytes_accessed=1600000, transcendentals=0),
    )(ring)


def gathered(value):
    parts = value.shape[0] // CUT
    pieces, held = [value], [value[n * parts : (n + 1) * parts] for n in range(CUT)]
    for hop in range(1, 5):
        for n in range(CUT):
            piece = meet(held[n], "y", hop % 2 == 0)
            held[n] = jnp.stack([held[n], piece]) if hop == 1 else piece
            pieces.append(piece)
    return pieces


def layer(tokens, route_ids, route_logits, norm_gain, gate_weight, up_weight, down_weight):
    experts = gate_weight.shape[0]
    x, c = lax.axis_index("x"), lax.axis_index("c")
    place = jnp.stack([x, c, lax.axis_index("y")]).astype(jnp.int32)
    packed = fold(norm_gain, gate_weight, up_weight, down_weight)
    slab = lax.all_to_all(packed, "z", split_axis=0, concat_axis=0, tiled=True)
    slabs = gathered(slab)

    sent = dispatch(place, route_ids.T, tokens, experts).reshape(experts, CAP, -1)
    arrived = lax.all_to_all(sent, "z", split_axis=0, concat_axis=0, tiled=True)
    mine = arrived.reshape(-1, arrived.shape[2])
    theirs = swap(mine)

    gate_new, up_new, down_new, down, hidden, send = expert(place, mine, theirs, slabs)
    received = swap(send)
    own, send = blocks(far_kernel, (2, 2), place, hidden, down)
    count = hidden.shape[0] // CUT
    cuts = [slice(n * count, (n + 1) * count) for n in range(CUT)]
    first = own.astype(F32) + received.astype(F32)
    came = []
    for cut in cuts:
        came.append(meet(first[:, cut].astype(BF16), "x", True))
    received = swap(send)
    (own,) = blocks(rest_kernel, (2,), place, hidden, down)
    last = []
    for n in range(CUT):
        kernel = functools.partial(onward_kernel, n * count)
        onward = added(kernel, count, own, received, came[n])
        last.append(meet(onward, "x", False))
    share = added(finish_kernel, CUT * count, own, received, *came, *last)
    back = lax.all_to_all(
        share.reshape(experts, CAP, 256), "z", split_axis=0, concat_axis=0, tiled=True
    ).reshape(-1, 256)
    mixed = combine(plan(route_ids, route_logits), back)
    ring = lax.all_gather(mixed, ("x", "c"), axis=0, tiled=False)
    mixed = assemble(ring)
    shape = (1, 2048, 256)
    return (mixed, gate_new.reshape(shape), up_new.reshape(shape), down_new.reshape(shape))


def solution(mesh):
    grid = Mesh(mesh.devices.reshape(8, 8, 4, 2), ("z", "y", "x", "c"))
    fs, tp = ("z", "y"), ("x", "c")
    return jax.shard_map(
        layer,
        mesh=grid,
        in_specs=(
            P(fs, None),
            P(fs, None),
            P(fs, None),
            P(fs),
            P(None, fs, tp),
            P(None, fs, tp),
            P(None, fs, tp),
        ),
        out_specs=(P(fs, None), P(fs, None, tp), P(fs, None, tp), P(fs, None, tp)),
        check_vma=False,
    )
```

```python
import functools

import jax
import jax.numpy as jnp
from jax import lax
from jax.experimental import pallas as pl
from jax.experimental.pallas import tpu as pltpu
from jax.sharding import Mesh
from jax.sharding import PartitionSpec as P


CAP = 96
CUT = 2
BF16 = jnp.bfloat16
F32 = jnp.float32
VMEM = pl.BlockSpec(memory_space=pltpu.VMEM)
SMEM = pl.BlockSpec(memory_space=pltpu.SMEM)
HBM = pl.BlockSpec(memory_space=pltpu.HBM)


def meet(value, axis, late):
    size = lax.axis_size(axis)
    pairs = []
    for i in range(size):
        for core in range(2):
            step = (1 - 2 * ((i + core) % 2)) * (-1 if late else 1)
            pairs.append((2 * i + core, 2 * ((i + step) % size) + core))
    return lax.ppermute(value, (axis, "c"), pairs)


def swap(value):
    return lax.ppermute(value, "c", [(0, 1), (1, 0)])


def fold_kernel(gain_ref, gate_ref, up_ref, down_ref, out_ref, gain_buf, buffers, sems):
    copies = [pltpu.make_async_copy(gain_ref, gain_buf, sems.at[3])]
    for k, ref in enumerate((gate_ref, up_ref, down_ref)):
        copies.append(pltpu.make_async_copy(ref, buffers.at[k], sems.at[k]))
    for copy in copies:
        copy.start()
    for copy in copies[:2]:
        copy.wait()
    size = gain_ref.shape[1]
    row = lax.broadcasted_iota(jnp.int32, (size, size), 0)
    column = lax.broadcasted_iota(jnp.int32, (size, size), 1)
    gain = jnp.sum(jnp.where(row == column, gain_buf[...], 0.0), axis=1, keepdims=True)
    for e in range(out_ref.shape[0]):
        out_ref[e, 0] = (gain * buffers[0, e]).astype(BF16)
    copies[2].wait()
    for e in range(out_ref.shape[0]):
        out_ref[e, 1] = (gain * buffers[1, e]).astype(BF16)
    copies[3].wait()
    for e in range(out_ref.shape[0]):
        out_ref[e, 2] = buffers[2, e].astype(BF16)


def fold(gain, gate, up, down):
    experts, rows, columns = gate.shape
    return pl.pallas_call(
        fold_kernel,
        out_shape=jax.ShapeDtypeStruct((experts, 3, rows, columns), BF16),
        in_specs=[HBM] * 4,
        out_specs=VMEM,
        scratch_shapes=[
            pltpu.VMEM((1, rows), F32),
            pltpu.VMEM((3, experts, rows, columns), F32),
            pltpu.SemaphoreType.DMA((4,)),
        ],
        name="fold",
        cost_estimate=pl.CostEstimate(flops=500_000_000, bytes_accessed=1200000, transcendentals=0),
    )(gain.reshape(1, rows), gate, up, down)


def dispatch_kernel(experts, place, ids_ref, tokens_ref, out_ref):
    rows = tokens_ref.shape[0]
    values = tokens_ref[...].astype(F32)
    center = jnp.mean(values, axis=1, keepdims=True)
    spread = jnp.mean(jnp.square(values - center), axis=1, keepdims=True)
    width = out_ref.shape[1]
    start = pl.multiple_of(place[1] * width, width)
    own = tokens_ref[:, pl.ds(start, width)].astype(F32)
    normed = ((own - center) * lax.rsqrt(spread + 1e-06)).astype(BF16)
    first, second = ids_ref[0:1, :], ids_ref[1:2, :]
    expert = lax.broadcasted_iota(jnp.int32, (experts, rows), 0)
    chosen = jnp.where((expert == first) | (expert == second), 1.0, 0.0)
    earlier = jnp.where(
        lax.broadcasted_iota(jnp.int32, (rows, rows), 0)
        < lax.broadcasted_iota(jnp.int32, (rows, rows), 1),
        1.0,
        0.0,
    )
    rank = jnp.dot(chosen.astype(BF16), earlier.astype(BF16), preferred_element_type=F32)
    slots = (rank + 0.5).astype(jnp.int32) + expert * CAP
    dest0 = jnp.sum(jnp.where(expert == first, slots, 0), axis=0, keepdims=True)
    dest1 = jnp.sum(jnp.where(expert == second, slots, 0), axis=0, keepdims=True)
    slot = lax.broadcasted_iota(jnp.int32, (experts * CAP, rows), 0)
    picks = jnp.where((slot == dest0) | (slot == dest1), 1.0, 0.0).astype(BF16)
    out_ref[...] = jnp.dot(picks, normed, preferred_element_type=F32).astype(BF16)


def dispatch(place, ids, tokens, experts):
    return pl.pallas_call(
        functools.partial(dispatch_kernel, experts),
        out_shape=jax.ShapeDtypeStruct((experts * CAP, tokens.shape[1] // 2), BF16),
        in_specs=[SMEM, VMEM, VMEM],
        out_specs=VMEM,
        compiler_params=pltpu.CompilerParams(vmem_limit_bytes=16 * 1024 * 1024),
        name="dispatch",
        cost_estimate=pl.CostEstimate(flops=2_000_000_000, bytes_accessed=1200000, transcendentals=0),
    )(place, ids, tokens)


def plan_kernel(ids_ref, logits_ref, out_ref):
    rows = ids_ref.shape[0]
    first, second = ids_ref[:, 0:1], ids_ref[:, 1:2]
    expert = lax.broadcasted_iota(jnp.int32, (rows, 128), 1)
    chosen = jnp.where((expert == first) | (expert == second), 1.0, 0.0)
    earlier = jnp.where(
        lax.broadcasted_iota(jnp.int32, (rows, rows), 1)
        < lax.broadcasted_iota(jnp.int32, (rows, rows), 0),
        1.0,
        0.0,
    )
    rank = jnp.dot(earlier.astype(BF16), chosen.astype(BF16), preferred_element_type=F32)
    slots = rank + (expert * CAP).astype(F32)
    dest0 = jnp.sum(jnp.where(expert == first, slots, 0.0), axis=1, keepdims=True)
    dest1 = jnp.sum(jnp.where(expert == second, slots, 0.0), axis=1, keepdims=True)
    weight0 = jax.nn.sigmoid(logits_ref[:, 0:1] - logits_ref[:, 1:2])
    weight1 = jax.nn.sigmoid(logits_ref[:, 1:2] - logits_ref[:, 0:1])
    column = lax.broadcasted_iota(jnp.int32, (rows, 128), 1)
    out_ref[...] = jnp.where(
        column == 0,
        dest0,
        jnp.where(column == 1, dest1, jnp.where(column == 2, weight0, weight1)),
    )


def plan(ids, logits):
    return pl.pallas_call(
        plan_kernel,
        out_shape=jax.ShapeDtypeStruct((ids.shape[0], 128), F32),
        in_specs=[VMEM, VMEM],
        out_specs=VMEM,
        compiler_params=pltpu.CompilerParams(vmem_limit_bytes=4 * 1024 * 1024),
        name="plan",
        cost_estimate=pl.CostEstimate(flops=1_000_000_000, bytes_accessed=200000, transcendentals=0),
    )(ids, logits)


def lowered(hidden, down, x, side, out, which):
    ahead = 1 - 2 * lax.rem(x + side, 2)
    offsets = (0, ahead, 2, -ahead)
    for j, k in enumerate(which):
        part = down[pl.ds(side * 4 + lax.rem(x + 4 + offsets[k], 4), 1)].reshape(256, 256)
        out[j] = lax.dot_general(
            hidden[...], part, (((1,), (1,)), ((), ())), preferred_element_type=F32
        ).astype(BF16)


def prepare_kernel(place, mine, *refs):
    slabs = refs[: 1 + 4 * CUT]
    gate_out, up_out, down_out, down_ref, gate_rest, up_rest, gate_sum, up_sum = refs[1 + 4 * CUT :]
    c, y = place[1], place[2]
    step = 1 - 2 * lax.rem(y + c, 2)
    size = 8 // CUT
    for k, out in enumerate((gate_out, up_out, down_out)):
        out[:, pl.ds(y, 1)] = slabs[0][:, k : k + 1]
        for n in range(CUT):
            low = n * size
            for hop, offsets in enumerate(((1,), (-1, -2), (2, 3), (-3, -4))):
                slab = slabs[1 + hop * CUT + n]
                for m, offset in enumerate(offsets):
                    at = lax.rem(y + 8 + offset * step, 8)
                    piece = slab[:, k : k + 1] if hop == 0 else slab[m, :, k : k + 1]
                    out[low : low + size, pl.ds(at, 1)] = piece
    for out, rest, total in ((gate_out, gate_rest, gate_sum), (up_out, up_rest, up_sum)):
        held = out[pl.ds(c * 4, 4)].reshape(1024, 256)
        total[...] = jnp.dot(mine[...], held, preferred_element_type=F32)
        rest[...] = out[pl.ds((1 - c) * 4, 4)].reshape(1024, 256)
    down_ref[...] = down_out[...].reshape(8, 256, 256)


def prepare(place, mine, slabs):
    count = mine.shape[0]
    matrix = jax.ShapeDtypeStruct((8, 8, 32, 256), BF16)
    rest = jax.ShapeDtypeStruct((1024, 256), BF16)
    total = jax.ShapeDtypeStruct((count, 256), F32)
    down = jax.ShapeDtypeStruct((8, 256, 256), BF16)
    return pl.pallas_call(
        prepare_kernel,
        out_shape=(matrix, matrix, matrix, down, rest, rest, total, total),
        in_specs=[SMEM] + [VMEM] * (2 + 4 * CUT),
        out_specs=(VMEM,) * 8,
        compiler_params=pltpu.CompilerParams(vmem_limit_bytes=17 * 1024 * 1024),
        name="prepare",
        cost_estimate=pl.CostEstimate(flops=3_000_000_000, bytes_accessed=9000000, transcendentals=0),
    )(place, mine, *slabs)


def expert_kernel(place, theirs, down, gate_rest, up_rest, gate_sum, up_sum, hidden_ref, send_ref):
    rows = theirs[...]
    gate_act = gate_sum[...] + jnp.dot(rows, gate_rest[...], preferred_element_type=F32)
    up_act = up_sum[...] + jnp.dot(rows, up_rest[...], preferred_element_type=F32)
    hidden_ref[...] = (gate_act / (1.0 + jnp.exp(-gate_act)) * up_act).astype(BF16)
    lowered(hidden_ref, down, place[0], 1 - place[1], send_ref, (3, 2))


def expert(place, theirs, *held):
    count = theirs.shape[0]
    return pl.pallas_call(
        expert_kernel,
        out_shape=(
            jax.ShapeDtypeStruct((count, 256), BF16),
            jax.ShapeDtypeStruct((2, count, 256), BF16),
        ),
        in_specs=[SMEM] + [VMEM] * 6,
        out_specs=(VMEM,) * 2,
        compiler_params=pltpu.CompilerParams(vmem_limit_bytes=14 * 1024 * 1024),
        name="expert",
        cost_estimate=pl.CostEstimate(flops=3_000_000_000, bytes_accessed=6000000, transcendentals=0),
    )(place, theirs, *held)


def far_kernel(place, hidden, down, own, send):
    lowered(hidden, down, place[0], place[1], own, (3, 2))
    lowered(hidden, down, place[0], 1 - place[1], send, (1, 0))


def rest_kernel(place, hidden, down, own):
    lowered(hidden, down, place[0], place[1], own, (1, 0))


def blocks(kernel, counts, place, hidden, down):
    shapes = [jax.ShapeDtypeStruct((n,) + hidden.shape, BF16) for n in counts]
    return pl.pallas_call(
        kernel,
        out_shape=shapes,
        in_specs=[SMEM, VMEM, VMEM],
        out_specs=[VMEM] * len(counts),
        compiler_params=pltpu.CompilerParams(vmem_limit_bytes=8 * 1024 * 1024),
        cost_estimate=pl.CostEstimate(flops=1_000_000_000, bytes_accessed=1500000, transcendentals=0),
    )(place, hidden, down)


def onward_kernel(low, own, received, came, out):
    rows = pl.ds(low, out.shape[0])
    total = own[0, rows].astype(F32) + received[0, rows].astype(F32) + came[1].astype(F32)
    out[...] = total.astype(BF16)


def finish_kernel(own, received, *refs):
    came, last, out = refs[:CUT], refs[CUT : 2 * CUT], refs[2 * CUT]
    size = out.shape[0] // CUT
    for n in range(CUT):
        rows = pl.ds(n * size, size)
        total = own[1, rows].astype(F32) + received[1, rows].astype(F32)
        total = total + came[n][0].astype(F32) + last[n][...].astype(F32)
        out[rows] = total.astype(BF16)


def added(kernel, rows, *args):
    return pl.pallas_call(
        kernel,
        out_shape=jax.ShapeDtypeStruct((rows, 256), BF16),
        in_specs=[VMEM] * len(args),
        out_specs=VMEM,
        compiler_params=pltpu.CompilerParams(vmem_limit_bytes=8 * 1024 * 1024),
        cost_estimate=pl.CostEstimate(flops=100_000_000, bytes_accessed=1500000, transcendentals=0),
    )(*args)


def combine_kernel(plan_ref, back_ref, out_ref):
    rows, slots = plan_ref.shape[0], back_ref.shape[0]
    slot = lax.broadcasted_iota(jnp.int32, (rows, slots), 1)
    back = back_ref[...]
    picked = []
    for k in range(2):
        dest = (plan_ref[:, k : k + 1] + 0.5).astype(jnp.int32)
        onehot = jnp.where(slot == dest, 1.0, 0.0).astype(BF16)
        picked.append(jnp.dot(onehot, back, preferred_element_type=F32))
    out_ref[...] = (plan_ref[:, 2:3] * picked[0] + plan_ref[:, 3:4] * picked[1]).astype(BF16)


def combine(planned, back):
    return pl.pallas_call(
        combine_kernel,
        out_shape=jax.ShapeDtypeStruct((planned.shape[0], 256), BF16),
        in_specs=[VMEM, VMEM],
        out_specs=VMEM,
        compiler_params=pltpu.CompilerParams(vmem_limit_bytes=6 * 1024 * 1024),
        name="combine",
        cost_estimate=pl.CostEstimate(flops=1_000_000_000, bytes_accessed=600000, transcendentals=0),
    )(planned, back)


def assemble_kernel(ring_ref, out_ref):
    for x in range(4):
        for c in range(2):
            low = (c * 4 + x) * 256
            out_ref[:, low : low + 256] = ring_ref[2 * x + c]


def assemble(ring):
    rows = ring.shape[1]
    return pl.pallas_call(
        assemble_kernel,
        out_shape=jax.ShapeDtypeStruct((rows, 2048), BF16),
        in_specs=[VMEM],
        out_specs=VMEM,
        compiler_params=pltpu.CompilerParams(vmem_limit_bytes=6 * 1024 * 1024),
        name="assemble",
        cost_estimate=pl.CostEstimate(flops=100_000_000, bytes_accessed=1600000, transcendentals=0),
    )(ring)


def gathered(value):
    parts = value.shape[0] // CUT
    pieces, held = [value], [value[n * parts : (n + 1) * parts] for n in range(CUT)]
    for hop in range(1, 5):
        for n in range(CUT):
            piece = meet(held[n], "y", hop % 2 == 0)
            held[n] = jnp.stack([held[n], piece]) if hop == 1 else piece
            pieces.append(piece)
    return pieces


def layer(tokens, route_ids, route_logits, norm_gain, gate_weight, up_weight, down_weight):
    experts = gate_weight.shape[0]
    x, c = lax.axis_index("x"), lax.axis_index("c")
    place = jnp.stack([x, c, lax.axis_index("y")]).astype(jnp.int32)
    packed = fold(norm_gain, gate_weight, up_weight, down_weight)
    slab = lax.all_to_all(packed, "z", split_axis=0, concat_axis=0, tiled=True)
    slabs = gathered(slab)

    sent = dispatch(place, route_ids.T, tokens, experts).reshape(experts, CAP, -1)
    arrived = lax.all_to_all(sent, "z", split_axis=0, concat_axis=0, tiled=True)
    mine = arrived.reshape(-1, arrived.shape[2])
    theirs = swap(mine)

    gate_new, up_new, down_new, down, *held = prepare(place, mine, slabs)
    hidden, send = expert(place, theirs, down, *held)
    received = swap(send)
    own, send = blocks(far_kernel, (2, 2), place, hidden, down)
    count = hidden.shape[0] // CUT
    cuts = [slice(n * count, (n + 1) * count) for n in range(CUT)]
    first = own.astype(F32) + received.astype(F32)
    came = []
    for cut in cuts:
        came.append(meet(first[:, cut].astype(BF16), "x", True))
    received = swap(send)
    (own,) = blocks(rest_kernel, (2,), place, hidden, down)
    last = []
    for n in range(CUT):
        kernel = functools.partial(onward_kernel, n * count)
        onward = added(kernel, count, own, received, came[n])
        last.append(meet(onward, "x", False))
    share = added(finish_kernel, CUT * count, own, received, *came, *last)
    back = lax.all_to_all(
        share.reshape(experts, CAP, 256), "z", split_axis=0, concat_axis=0, tiled=True
    ).reshape(-1, 256)
    mixed = combine(plan(route_ids, route_logits), back)
    ring = lax.all_gather(lax.all_gather(mixed, "c", axis=0, tiled=False), "x", axis=0, tiled=False)
    ring = ring.reshape((8,) + mixed.shape)
    mixed = assemble(ring)
    shape = (1, 2048, 256)
    return (mixed, gate_new.reshape(shape), up_new.reshape(shape), down_new.reshape(shape))


def solution(mesh):
    grid = Mesh(mesh.devices.reshape(8, 8, 4, 2), ("z", "y", "x", "c"))
    fs, tp = ("z", "y"), ("x", "c")
    return jax.shard_map(
        layer,
        mesh=grid,
        in_specs=(
            P(fs, None),
            P(fs, None),
            P(fs, None),
            P(fs),
            P(None, fs, tp),
            P(None, fs, tp),
            P(None, fs, tp),
        ),
        out_specs=(P(fs, None), P(fs, None, tp), P(fs, None, tp), P(fs, None, tp)),
        check_vma=False,
    )
```
